512 devices in a mesh: ep: 128 (over z, x, core), tp: 4 (over y).
Axes of the slice: x: 4, y: 4, z: 16, core: 2. Of those that a mesh axis runs over, the one named last changes fastest.
Arguments:
- tokens: bfloat16 [1024, 1024], P('ep'), may hold values from -6 to 6
- lengths: int32 [1024], P('ep'), may hold values from 1 to 512, as said below
- cache_keys: bfloat16 [1024, 512, 4, 128], P('ep', None, 'tp'), may hold values from -2.5 to 2.5
- cache_values: bfloat16 [1024, 512, 4, 128], P('ep', None, 'tp'), may hold values from -6 to 6
- cache_cum: float32 [1024, 4, 512], P('ep', 'tp'), may hold values from -1536 to 0, as said below
- norm_gain: bfloat16 [1024], replicated, may hold values from 0.099609375 to 1.8984375
- query_weight: bfloat16 [1024, 1024], P(None, 'tp'), may hold values from -0.1875 to 0.1875
- key_weight: bfloat16 [1024, 512], P(None, 'tp'), may hold values from -0.1875 to 0.1875
- value_weight: bfloat16 [1024, 512], P(None, 'tp'), may hold values from -0.1875 to 0.1875
- forget_weight: bfloat16 [1024, 4], P(None, 'tp'), may hold values from -0.1875 to 0.1875
- forget_bias: float32 [4], P('tp'), may hold values from -1 to 2
- query_gain: bfloat16 [128], replicated, may hold values from 0.29882812 to 2.5
- key_gain: bfloat16 [128], replicated, may hold values from 0.099609375 to 1.8984375
- out_weight: bfloat16 [1024, 1024], P('tp'), may hold values from -0.1875 to 0.1875
- ffn_gain: bfloat16 [1024], replicated, may hold values from 0.099609375 to 1.8984375
- mix_weight: bfloat16 [1024], replicated, may hold values from -0.1875 to 0.1875
- shared_gate: bfloat16 [1024, 4096], P(None, 'ep'), may hold values from -0.1875 to 0.1875
- shared_up: bfloat16 [1024, 4096], P(None, 'ep'), may hold values from -0.1875 to 0.1875
- shared_down: bfloat16 [4096, 1024], P('ep', 'tp'), may hold values from -0.09375 to 0.09375
- routes: int32 [1024, 2], P('ep'), may hold values from 0 to 127, all different within a row; in each aligned block of 8 rows (0 to 7, 8 to 15, ...) at most 4 rows name the same one
- route_weights: float32 [1024, 2], P('ep'), may hold values from 0.1 to 1
- expert_gate: bfloat16 [128, 1024, 512], P('ep', None, 'tp'), may hold values from -0.1875 to 0.1875
- expert_up: bfloat16 [128, 1024, 512], P('ep', None, 'tp'), may hold values from -0.1875 to 0.1875
- expert_down: bfloat16 [128, 512, 1024], P('ep', 'tp'), may hold values from -0.25 to 0.25
Outputs:
- layer_out: bfloat16 [1024, 1024], P('ep', 'tp')
The draws below stay inside these ranges and needn't reach their ends.
Inputs may be any that keep to these rules, and one draw needn't show every extreme that they name: `lengths`: at least one sequence has exactly 512 cached positions. `cache_cum`: along the positions each row never rises. `routes`: the 2 experts of a token differ; among the 8 rows of one device no expert is named by more than 4 rows, a bound that some block reaches.
All inputs are finite; a program needn't handle non-finite values.
Results may differ from the reference program's by a relative error of at most 0.013.
Values may be sent and summed in bfloat16 or wider, within the bound.
No kernel may reach another device: no remote copies, remote signals or barrier semaphores. Data moves between devices by JAX's collectives and lax.ppermute only.
A program may use at most 64 MiB of HBM per device.

```python
import math
import jax
import jax.numpy as jnp
import numpy as np
from jax import lax

D = 1024
HEADS = 8
KV_HEADS = 4
HEAD = 128
FE = 512
FS = 4096
TOPK = 2
CAP = 4
SEQ_DEV = 8
CACHE = 512
SEQS = 1024
EXPERTS = 128
N_TP = 4


def draw_lengths(key, part):
    key_levels, key_lengths, key_chosen = jax.random.split(key, 3)
    blocks = SEQS // SEQ_DEV
    levels = jax.random.randint(key_levels, (blocks, 1), 1, 5)
    ceiling = CACHE * levels // 4
    drawn_lengths = jax.random.randint(key_lengths, (blocks, SEQ_DEV), 0, ceiling) + 1
    chosen = jax.random.randint(key_chosen, (), 0, SEQS)
    flat_lengths = drawn_lengths.reshape(-1)
    return jnp.where(jnp.arange(SEQS) == chosen, CACHE, flat_lengths).astype(jnp.int32)


def draw_cache_cum(key, part):
    key_slow, key_fast, key_seq, key_block, key_step = jax.random.split(key, 5)
    picks = jax.random.randint(key_slow, (SEQS, KV_HEADS, 1), 0, 10)
    slow_heads = picks < 5
    fast_span = float(min(30, max(CACHE // 8, 2)))
    fast_rate = 1.0 / jax.random.uniform(key_fast, (SEQS, KV_HEADS, 1), jnp.float32, fast_span, 2.0 * fast_span)
    decay_rate = jnp.where(slow_heads, 2.0 / CACHE, fast_rate)
    seq_factor = jnp.exp(jax.random.uniform(key_seq, (SEQS, 1, 1), jnp.float32, -0.69, 0.69))
    block_span = min(64, CACHE)
    block_factor = jax.random.uniform(key_block, (SEQS, KV_HEADS, CACHE // block_span, 1), jnp.float32, 0.5, 1.5)
    block_factor = jnp.broadcast_to(block_factor, (SEQS, KV_HEADS, CACHE // block_span, block_span))
    block_factor = block_factor.reshape(SEQS, KV_HEADS, CACHE)
    step_factor = jax.random.uniform(key_step, (SEQS, KV_HEADS, CACHE), jnp.float32, 0.5, 1.5)
    log_gate = -decay_rate * seq_factor * block_factor * step_factor
    return jnp.cumsum(log_gate, axis=-1).astype(jnp.float32)


def steps_of(rng, extent, shards, low, top_value):
    level = 1.0
    for dim, shards_of in shards:
        draws = jax.random.uniform(jax.random.fold_in(jax.random.fold_in(rng, 6), dim), (shards_of,), jnp.float32, low / len(shards), top_value / len(shards))
        level = level * jnp.repeat(jnp.exp(draws), extent[dim] // shards_of).reshape((-1,) + (1,) * (len(extent) - 1 - dim))
    return level


def shared_out(own_key, own, number, rows, amount, top, bound, skew):
    sequence = jax.random.permutation(own_key, amount)
    heavy_load, usual = load_shares(amount, rows * top, bound, skew, True), load_shares(amount, rows * top, bound, skew, False)
    places = jnp.arange(amount)

    def named(sizes, rotation):
        used = int((sizes > 0).sum())
        fixed = max(1, used // 4)
        moved = fixed + (places - fixed + rotation * (used - fixed)) % max(1, amount - fixed)
        return jnp.zeros((amount,), jnp.int32).at[sequence[jnp.where(places < fixed, places, moved)]].set(jnp.asarray(sizes, jnp.int32))

    sizes = jnp.where(number % 4 == 0, named(heavy_load, number // 4), named(usual, number - number // 4 - 1))
    mixed = jax.random.permutation(jax.random.fold_in(own, 3), amount)
    giver, taker = mixed[0:amount // 2 * 2:2], mixed[1:amount // 2 * 2:2]
    margin = jnp.minimum(sizes[giver] - 1, bound - sizes[taker]) // 2
    margin = jnp.where((giver == sequence[0]) | (taker == sequence[0]) | (sizes[taker] == 0), 0, jnp.maximum(margin, 0))
    moved = jax.random.randint(jax.random.fold_in(own, 4), (amount // 2,), 0, 1 << 20) % (margin + 1)
    sizes = sizes.at[giver].add(-moved).at[taker].add(moved)
    members = jnp.searchsorted(jnp.cumsum(sizes), jnp.arange(rows * top), side="right").astype(jnp.int32)
    grid = members.reshape(top, rows).T
    grid = grid[jax.random.permutation(jax.random.fold_in(own, 1), rows)]
    rotation = jax.random.randint(jax.random.fold_in(own, 2), (rows, 1), 0, top)
    return jnp.take_along_axis(grid, (jnp.arange(top)[None, :] + rotation) % top, axis=1)


def load_shares(number_of, total, reach, lean, full):
    portions = [(1 << 20) // math.isqrt(standing ** lean) + 1 for standing in range(1, number_of + 1)]
    largest = reach if full else min(reach, max(-(-total // number_of), total * portions[0] // sum(portions)))
    least = 1 if total - largest >= number_of - 1 else 0
    counts, spare = [largest] + [least] * (number_of - 1), total - largest - least * (number_of - 1)
    while spare > 0:
        movable = [i for i in range(1, number_of) if counts[i] < largest] or [i for i in range(1, number_of) if counts[i] < reach]
        whole, remaining = sum([portions[i] for i in movable]), spare
        for i in movable:
            more = min(reach - counts[i], max(1, remaining * portions[i] // whole), spare)
            counts[i] = counts[i] + more
            spare = spare - more
    return np.array(counts)


def normal_values(own_key, extent, width, limit, cuts=(), kind=jnp.bfloat16):
    factor_of = steps_of(own_key, extent, cuts, -0.22, 0.18) if cuts else 1.0
    array = jax.random.normal(own_key, extent, jnp.float32) * width * factor_of
    return jnp.minimum(jnp.maximum(array, -limit), limit).astype(kind)


def setup_inputs(seed: int = 0) -> dict:
    key_of = jax.random.split(jax.random.key(seed), 25)
    tokens = normal_values(key_of[0], (SEQS, D), 1.0, 6.0, ((0, 128),))
    lengths = draw_lengths(jax.random.fold_in(key_of[24], 71), 0)
    cache_keys = normal_values(key_of[2], (SEQS, CACHE, KV_HEADS, HEAD), 1.0, 2.5, ((0, 128), (2, 4)))
    cache_values = normal_values(key_of[3], (SEQS, CACHE, KV_HEADS, HEAD), 1.0, 6.0, ((0, 128), (2, 4)))
    cache_cum = draw_cache_cum(jax.random.fold_in(key_of[24], 71), 0)
    norm_gain = jnp.clip(1.0 + 0.18 * jax.random.normal(key_of[5], (D,), jnp.float32), 0.099609375, 1.8984375).astype(jnp.bfloat16)
    query_weight = normal_values(key_of[6], (D, HEADS * HEAD), D ** -0.5, 0.1875, ((1, 4),))
    key_weight = normal_values(key_of[7], (D, KV_HEADS * HEAD), D ** -0.5, 0.1875, ((1, 4),))
    value_weight = normal_values(key_of[8], (D, KV_HEADS * HEAD), D ** -0.5, 0.1875, ((1, 4),))
    forget_weight = normal_values(key_of[9], (D, KV_HEADS), D ** -0.5, 0.1875, ((1, 4),))
    forget_bias = jnp.clip(-1.0 + 3.0 * jax.random.uniform(key_of[10], (KV_HEADS,), jnp.float32) ** steps_of(key_of[10], (KV_HEADS,), ((0, 4),), -0.2, 0.2), -1.0, 2.0)
    query_gain = jnp.clip(jnp.exp(jax.random.uniform(key_of[11], (HEAD,), jnp.float32, math.log(0.29882812), math.log(2.5))), 0.29882812, 2.5).astype(jnp.bfloat16)
    key_gain = jnp.clip(1.0 + 0.18 * jax.random.normal(key_of[12], (HEAD,), jnp.float32), 0.099609375, 1.8984375).astype(jnp.bfloat16)
    out_weight = normal_values(key_of[13], (HEADS * HEAD, D), (HEADS * HEAD) ** -0.5, 0.1875, ((0, 4),))
    ffn_gain = jnp.clip(1.0 + 0.18 * jax.random.normal(key_of[14], (D,), jnp.float32), 0.099609375, 1.8984375).astype(jnp.bfloat16)
    mix_weight = normal_values(key_of[15], (D,), D ** -0.5, 0.1875)
    shared_gate = normal_values(key_of[16], (D, FS), D ** -0.5, 0.1875, ((1, 128),))
    shared_up = normal_values(key_of[17], (D, FS), D ** -0.5, 0.1875, ((1, 128),))
    shared_down = normal_values(key_of[18], (FS, D), FS ** -0.5, 0.09375, ((0, 128), (1, 4)))
    routes_keys = jax.random.split(jax.random.fold_in(key_of[19], 1), SEQS // SEQ_DEV)
    routes_turns = jax.random.permutation(jax.random.fold_in(key_of[19], 3), SEQS // SEQ_DEV)
    routes = jax.vmap(lambda own, number: shared_out(jax.random.fold_in(key_of[19], 2), own, number, SEQ_DEV, EXPERTS, TOPK, CAP, 2))(routes_keys, routes_turns).reshape((SEQS, TOPK))
    route_weights = jnp.clip(jnp.exp(math.log(1.0) - 2.3025851 * jax.random.uniform(key_of[20], (SEQS, TOPK), jnp.float32) ** steps_of(key_of[20], (SEQS, TOPK), ((0, 128),), -0.2, 0.2)), 0.1, 1.0)
    expert_gate = normal_values(key_of[21], (EXPERTS, D, FE), D ** -0.5, 0.1875, ((0, 128), (2, 4)))
    expert_up = normal_values(key_of[22], (EXPERTS, D, FE), D ** -0.5, 0.1875, ((0, 128), (2, 4)))
    expert_down = normal_values(key_of[23], (EXPERTS, FE, D), FE ** -0.5, 0.25, ((0, 128), (1, 4)))
    return dict(tokens=tokens, lengths=lengths, cache_keys=cache_keys, cache_values=cache_values, cache_cum=cache_cum, norm_gain=norm_gain, query_weight=query_weight, key_weight=key_weight, value_weight=value_weight, forget_weight=forget_weight, forget_bias=forget_bias, query_gain=query_gain, key_gain=key_gain, out_weight=out_weight, ffn_gain=ffn_gain, mix_weight=mix_weight, shared_gate=shared_gate, shared_up=shared_up, shared_down=shared_down, routes=routes, route_weights=route_weights, expert_gate=expert_gate, expert_up=expert_up, expert_down=expert_down)


epsilon = 1e-06

def rms_norm(values, gain):
    values = values.astype(jnp.float32)
    return values * lax.rsqrt(lax.optimization_barrier(jnp.mean(values * values, axis=-1, keepdims=True)) + epsilon) * gain.astype(jnp.float32)

def attend(inputs):
    query_one, key_one, value_one, log_one, keys_one, values_one, cum_one, length_one = inputs
    position = jnp.arange(CACHE, dtype=jnp.int32)
    live = position < length_one
    last_cum = lax.optimization_barrier(jnp.sum(jnp.where(position[None, :] == length_one - 1, cum_one, 0.0), axis=-1))
    gate_bias = last_cum[:, None] - cum_one + log_one[:, None]
    score_scale = HEAD ** (-0.5)
    past = jnp.einsum('kgd,pkd->kgp', query_one.astype(jnp.float32), keys_one.astype(jnp.float32)) * score_scale
    past = past + gate_bias[:, None, :]
    past = jnp.where(live[None, None, :], past, -jnp.inf)
    own = lax.optimization_barrier(jnp.sum(query_one.astype(jnp.float32) * key_one.astype(jnp.float32)[:, None, :], axis=-1)) * score_scale
    past_exp = jnp.exp(past)
    own_exp = jnp.exp(own)
    denominator = lax.optimization_barrier(jnp.sum(past_exp, axis=-1)) + own_exp
    past_prob = (past_exp / denominator[..., None]).astype(jnp.bfloat16)
    own_prob = (own_exp / denominator).astype(jnp.bfloat16)
    mixed = jnp.einsum('kgp,pkd->kgd', past_prob.astype(jnp.float32), values_one.astype(jnp.float32))
    mixed = mixed + own_prob.astype(jnp.float32)[..., None] * value_one.astype(jnp.float32)[:, None, :]
    return mixed.astype(jnp.bfloat16)

def reference(tokens, lengths, cache_keys, cache_values, cache_cum, norm_gain, query_weight, key_weight, value_weight, forget_weight, forget_bias, query_gain, key_gain, out_weight, ffn_gain, mix_weight, shared_gate, shared_up, shared_down, routes, route_weights, expert_gate, expert_up, expert_down):
    seq_count = tokens.shape[0]
    normed = rms_norm(tokens, norm_gain).astype(jnp.bfloat16)
    query = jnp.dot(normed, query_weight, preferred_element_type=jnp.float32)
    query = rms_norm(query.reshape(seq_count, KV_HEADS, HEADS // KV_HEADS, HEAD), query_gain).astype(jnp.bfloat16)
    new_key = jnp.dot(normed, key_weight, preferred_element_type=jnp.float32)
    new_key = rms_norm(new_key.reshape(seq_count, KV_HEADS, HEAD), key_gain).astype(jnp.bfloat16)
    new_value = jnp.dot(normed, value_weight, preferred_element_type=jnp.float32).astype(jnp.bfloat16)
    new_value = new_value.reshape(seq_count, KV_HEADS, HEAD)
    new_log = jax.nn.log_sigmoid(jnp.dot(normed, forget_weight, preferred_element_type=jnp.float32) + forget_bias)
    heads_out = lax.map(attend, (query, new_key, new_value, new_log, cache_keys, cache_values, cache_cum, lengths))
    heads_out = heads_out.reshape(seq_count, N_TP, -1)
    partial_value = jnp.einsum('btf,tfd->btd', heads_out.astype(jnp.float32), out_weight.reshape(N_TP, -1, D).astype(jnp.float32)).astype(jnp.bfloat16)
    attended = lax.optimization_barrier(jnp.sum(partial_value.astype(jnp.float32), axis=1))
    residual = tokens.astype(jnp.float32) + attended
    ffn_in = rms_norm(residual, ffn_gain).astype(jnp.bfloat16)
    mix_gate = jax.nn.sigmoid(jnp.dot(ffn_in, mix_weight, preferred_element_type=jnp.float32))
    pre_gate = jnp.dot(ffn_in, shared_gate, preferred_element_type=jnp.float32)
    pre_up = jnp.dot(ffn_in, shared_up, preferred_element_type=jnp.float32)
    shared_hidden = (jax.nn.silu(pre_gate) * pre_up).astype(jnp.bfloat16)
    dense = jnp.dot(shared_hidden, shared_down, preferred_element_type=jnp.float32)
    norm_weights = route_weights / lax.optimization_barrier(jnp.sum(route_weights, axis=1, keepdims=True))

    def expert_row(inputs):
        row, chosen, weights = inputs
        total = jnp.zeros((D,), jnp.float32)
        for route_slot in range(TOPK):
            index = chosen[route_slot]
            gate_mat = expert_gate[index]
            up_mat = expert_up[index]
            down_mat = expert_down[index]
            hidden = jax.nn.silu(jnp.dot(row, gate_mat, preferred_element_type=jnp.float32))
            hidden = (hidden * jnp.dot(row, up_mat, preferred_element_type=jnp.float32)).astype(jnp.bfloat16)
            parts = jnp.einsum('tf,tfd->td', hidden.reshape(N_TP, -1).astype(jnp.float32), down_mat.reshape(N_TP, -1, D).astype(jnp.float32)).astype(jnp.bfloat16)
            expert_out = lax.optimization_barrier(jnp.sum(parts.astype(jnp.float32), axis=0)).astype(jnp.bfloat16)
            total = total + weights[route_slot] * expert_out.astype(jnp.float32)
        return total
    routed = lax.map(expert_row, (ffn_in, routes, norm_weights))
    return (residual + mix_gate[:, None] * dense + routed).astype(jnp.bfloat16)
```

```python
import jax
import jax.numpy as jnp
from jax import lax
from jax.sharding import Mesh
from jax.sharding import PartitionSpec as P

EP = ("ep_0", "ep_1", "ep_2")
PAIR = "ep_2"
LANES = 128


epsilon = 1e-06


def copy_for_each(shard, axis):
    peers = lax.axis_size(axis)
    return lax.all_to_all(
        jnp.broadcast_to(shard[None], (peers, *shard.shape)), axis, 0, 0, tiled=True
    )


def swap(shard):
    return lax.ppermute(shard, PAIR, [(0, 1), (1, 0)])


def lane_blocks(weight):
    rows, columns = weight.shape
    return jnp.concatenate(jnp.split(weight, columns // LANES, axis=1), axis=0)


def wide_rows(blocks, rows):
    peers = blocks.shape[0]
    blocks = blocks.reshape(peers, -1, rows, LANES)
    return jnp.moveaxis(blocks, 2, 1).reshape(peers, rows, -1)


def pair_of(values, member):
    split = values.reshape(2, -1, values.shape[-1])
    return lax.dynamic_index_in_dim(split, member, 1, keepdims=False)


def rms_norm(values, gain):
    values = values.astype(jnp.float32)
    return (
        values
        * lax.rsqrt(jnp.mean(values * values, axis=-1, keepdims=True) + epsilon)
        * gain.astype(jnp.float32)
    )


def per_device(
    tokens,
    lengths,
    cache_keys,
    cache_values,
    cache_cum,
    norm_gain,
    query_weight,
    key_weight,
    value_weight,
    forget_weight,
    forget_bias,
    query_gain,
    key_gain,
    out_weight,
    ffn_gain,
    mix_weight,
    shared_gate,
    shared_up,
    shared_down,
    routes,
    route_weights,
    expert_gate,
    expert_up,
    expert_down,
):
    seq_rows = tokens.shape[0]
    cache_len = cache_keys.shape[1]
    kv_local = cache_keys.shape[2]
    head_size = cache_keys.shape[3]
    normed = rms_norm(tokens, norm_gain).astype(jnp.bfloat16)
    query = jnp.dot(normed, query_weight, preferred_element_type=jnp.float32)
    query = rms_norm(query.reshape(seq_rows, kv_local, -1, head_size), query_gain).astype(
        jnp.bfloat16
    )
    new_key = jnp.dot(normed, key_weight, preferred_element_type=jnp.float32)
    new_key = rms_norm(new_key.reshape(seq_rows, kv_local, head_size), key_gain).astype(
        jnp.bfloat16
    )
    new_value = jnp.dot(normed, value_weight, preferred_element_type=jnp.float32).astype(
        jnp.bfloat16
    )
    new_value = new_value.reshape(seq_rows, kv_local, head_size)
    new_log = jax.nn.log_sigmoid(
        jnp.dot(normed, forget_weight, preferred_element_type=jnp.float32) + forget_bias
    )
    position = jnp.arange(cache_len, dtype=jnp.int32)
    live = position[None, :] < lengths[:, None]
    at_last = (position[None, :] == lengths[:, None] - 1)[:, None, :]
    last_cum = jnp.sum(jnp.where(at_last, cache_cum, 0.0), axis=-1)
    gate_bias = last_cum[:, :, None] - cache_cum + new_log[:, :, None]
    score_scale = head_size ** (-0.5)
    past = (
        jnp.einsum("skgd,spkd->skgp", query, cache_keys, preferred_element_type=jnp.float32)
        * score_scale
    )
    past = past + gate_bias[:, :, None, :]
    past = jnp.where(live[:, None, None, :], past, -jnp.inf)
    own = (
        jnp.sum(query.astype(jnp.float32) * new_key.astype(jnp.float32)[:, :, None, :], axis=-1)
        * score_scale
    )
    past_exp = jnp.exp(past)
    own_exp = jnp.exp(own)
    denominator = jnp.sum(past_exp, axis=-1) + own_exp
    past_prob = (past_exp / denominator[..., None]).astype(jnp.bfloat16)
    own_prob = (own_exp / denominator).astype(jnp.bfloat16)
    mixed = jnp.einsum(
        "skgp,spkd->skgd", past_prob, cache_values, preferred_element_type=jnp.float32
    )
    mixed = (
        mixed
        + own_prob.astype(jnp.float32)[..., None] * new_value.astype(jnp.float32)[:, :, None, :]
    )
    heads_out = mixed.astype(jnp.bfloat16).reshape(seq_rows, -1)
    partial_value = jnp.dot(heads_out, out_weight, preferred_element_type=jnp.float32)
    attended = copy_for_each(partial_value.astype(jnp.bfloat16), "tp")
    attended = jnp.sum(attended.astype(jnp.float32), axis=0)
    residual = tokens.astype(jnp.float32) + attended
    ffn_in = rms_norm(residual, ffn_gain).astype(jnp.bfloat16)

    member = lax.axis_index("tp")
    width = ffn_in.shape[1]
    hidden_local = expert_gate.shape[2]
    units = shared_gate.shape[1]
    pack = jnp.concatenate(
        [
            expert_gate[0],
            expert_up[0],
            lane_blocks(expert_down[0]),
            lane_blocks(shared_down),
        ],
        axis=0,
    )
    packs = copy_for_each(pack, "tp")
    packs = packs.reshape(-1, *pack.shape)
    gate_all = packs[:, :width]
    up_all = packs[:, width : 2 * width]
    down_end = 2 * width + hidden_local * width // LANES
    down_all = wide_rows(packs[:, 2 * width : down_end], hidden_local)
    shared_cols = wide_rows(packs[:, down_end:], units)
    shared_down_all = jnp.moveaxis(shared_cols, 0, 1).reshape(units, width)
    front = jnp.concatenate([shared_gate, shared_up, mix_weight[:, None]], axis=1)

    norm_weights = route_weights / jnp.sum(route_weights, axis=1, keepdims=True)
    high = norm_weights.astype(jnp.bfloat16)
    low = (norm_weights - high.astype(jnp.float32)).astype(jnp.bfloat16)
    notes = jnp.concatenate([routes.astype(jnp.bfloat16), high, low], axis=1)
    notes = jnp.pad(notes, ((0, 0), (0, LANES - notes.shape[1])))
    outgoing = pair_of(jnp.concatenate([ffn_in, notes], axis=1), member)
    peers = lax.axis_size(EP)
    outgoing = jnp.broadcast_to(outgoing[None], (peers // 2, *outgoing.shape))
    own_rows = lax.all_to_all(outgoing.reshape(peers, -1), EP, 0, 0, tiled=True)
    expert = lax.axis_index(EP).astype(jnp.float32)

    def share(rows):
        values = rows[:, :width]
        marks = rows[:, width:].astype(jnp.float32)
        picked = marks[:, 0:2] == expert
        weight = jnp.sum(jnp.where(picked, marks[:, 2:4] + marks[:, 4:6], 0.0), axis=1)
        pre = jnp.dot(values, front, preferred_element_type=jnp.float32)
        mix_gate = jax.nn.sigmoid(pre[:, 2 * units])
        shared = (jax.nn.silu(pre[:, :units]) * pre[:, units : 2 * units]).astype(jnp.bfloat16)
        dense = jnp.dot(shared, shared_down_all, preferred_element_type=jnp.float32)
        gate = jnp.einsum("nd,tdf->tnf", values, gate_all, preferred_element_type=jnp.float32)
        up = jnp.einsum("nd,tdf->tnf", values, up_all, preferred_element_type=jnp.float32)
        hidden = (jax.nn.silu(gate) * up).astype(jnp.bfloat16)
        routed = jnp.einsum("tnf,tfd->nd", hidden, down_all, preferred_element_type=jnp.float32)
        return mix_gate[:, None] * dense + weight[:, None] * routed

    pair_rows = swap(own_rows)
    pair_share = swap(share(pair_rows).astype(jnp.bfloat16))
    total = share(own_rows) + pair_share.astype(jnp.float32)
    total = total.astype(jnp.bfloat16).reshape(peers * lax.axis_size("tp"), -1)
    returned = lax.all_to_all(total, (*EP, "tp"), 0, 0, tiled=True)
    returned = returned.reshape(peers // 2, seq_rows, -1).astype(jnp.float32)
    slice_width = returned.shape[2]
    residual_slice = lax.dynamic_slice_in_dim(residual, member * slice_width, slice_width, 1)
    return (residual_slice + jnp.sum(returned, axis=0)).astype(jnp.bfloat16)


def solution(mesh):
    finer = Mesh(mesh.devices.reshape(16, 4, 2, mesh.shape["tp"]), ("ep_0", "ep_1", "ep_2", "tp"))
    placed = (
        P(EP, None),
        P(EP),
        P(EP, None, "tp", None),
        P(EP, None, "tp", None),
        P(EP, "tp", None),
        P(),
        P(None, "tp"),
        P(None, "tp"),
        P(None, "tp"),
        P(None, "tp"),
        P("tp"),
        P(),
        P(),
        P("tp", None),
        P(),
        P(),
        P(None, EP),
        P(None, EP),
        P(EP, "tp"),
        P(EP, None),
        P(EP, None),
        P(EP, None, "tp"),
        P(EP, None, "tp"),
        P(EP, "tp", None),
    )
    return jax.shard_map(
        per_device, mesh=finer, in_specs=placed, out_specs=P(EP, "tp"), check_vma=False
    )
```

```python
import jax
import jax.numpy as jnp
from jax import lax
from jax.experimental import pallas as pl
from jax.experimental.pallas import tpu as pltpu
from jax.sharding import Mesh
from jax.sharding import PartitionSpec as P

EP = ("ep_0", "ep_1", "ep_2")
PAIR = "ep_2"
LANES = 128
NOTE_ROWS = 2

epsilon = 1e-06

VMEM = pl.BlockSpec(memory_space=pltpu.VMEM)
SMEM = pl.BlockSpec(memory_space=pltpu.SMEM)
ANY = pl.BlockSpec(memory_space=pl.ANY)


def swap(shard):
    return lax.ppermute(shard, PAIR, [(0, 1), (1, 0)])


def scaled(values, gain):
    mean = jnp.mean(values * values, axis=-1, keepdims=True)
    return values * lax.rsqrt(mean + epsilon) * gain


def silu(values):
    return values / (1.0 + jnp.exp(-values))


def wide_dot(left, right):
    return jnp.dot(left, right, preferred_element_type=jnp.float32)


def attend_kernel(
    lengths,
    forget_bias,
    tokens,
    keys,
    values,
    cum,
    norm_gain,
    query_weight,
    key_weight,
    value_weight,
    forget_weight,
    query_gain,
    key_gain,
    out_weight,
    expert_gate,
    expert_up,
    expert_down,
    shared_down,
    partial,
    packed,
    sems,
):
    width = expert_gate.shape[0]
    copies = []

    def send(source, first):
        target = packed.at[pl.ds(first, source.shape[0]), :]
        copy = pltpu.make_async_copy(source, target, sems.at[len(copies)])
        copy.start()
        copies.append(copy)
        return first + source.shape[0]

    row = send(expert_gate, 0)
    row = send(expert_up, row)
    for block in range(width // LANES):
        row = send(expert_down.at[:, pl.ds(block * LANES, LANES)], row)
    for block in range(shared_down.shape[1] // LANES):
        row = send(shared_down.at[:, pl.ds(block * LANES, LANES)], row)

    seqs, cache_len, head = keys.shape
    groups = query_weight.shape[1] // head
    normed = scaled(tokens[...].astype(jnp.float32), norm_gain[...].astype(jnp.float32))
    normed = normed.astype(jnp.bfloat16)
    wide = wide_dot(normed, query_weight[...])
    gain = query_gain[...].astype(jnp.float32)
    query = [scaled(wide[:, g * head : (g + 1) * head], gain) for g in range(groups)]
    query = jnp.concatenate(query, axis=0).astype(jnp.bfloat16)
    new_key = scaled(wide_dot(normed, key_weight[...]), key_gain[...].astype(jnp.float32))
    new_key = new_key.astype(jnp.bfloat16).astype(jnp.float32)
    new_value = wide_dot(normed, value_weight[...]).astype(jnp.bfloat16).astype(jnp.float32)
    products = normed.astype(jnp.float32) * forget_weight[...].astype(jnp.float32)
    forget = jnp.sum(products, axis=-1, keepdims=True) + forget_bias[0]
    new_log = jnp.minimum(forget, 0.0) - jnp.log1p(jnp.exp(-jnp.abs(forget)))

    rows = groups * seqs
    owner = lax.broadcasted_iota(jnp.int32, (rows, cache_len), 0) % seqs
    position = lax.broadcasted_iota(jnp.int32, (rows, cache_len), 1)
    scores = jnp.zeros((rows, cache_len), jnp.float32)
    decay = jnp.zeros((rows, cache_len), jnp.float32)
    length = jnp.zeros((rows, cache_len), jnp.int32)
    for b in range(seqs):
        mine = owner == b
        one = lax.dot_general(
            query, keys[b], (((1,), (1,)), ((), ())), preferred_element_type=jnp.float32
        )
        scores = jnp.where(mine, one, scores)
        decay = jnp.where(mine, cum[b], decay)
        length = jnp.where(mine, lengths[b], length)
    last = jnp.where(position == length - 1, decay, 0.0)
    last = jnp.sum(last, axis=-1, keepdims=True)
    bias = last - decay + jnp.concatenate([new_log] * groups, axis=0)
    score_scale = head ** (-0.5)
    past = jnp.where(position < length, scores * score_scale + bias, -jnp.inf)
    own = query.astype(jnp.float32) * jnp.concatenate([new_key] * groups, axis=0)
    own = jnp.sum(own, axis=-1, keepdims=True) * score_scale
    past_exp = jnp.exp(past)
    own_exp = jnp.exp(own)
    denominator = jnp.sum(past_exp, axis=-1, keepdims=True) + own_exp
    past_prob = (past_exp / denominator).astype(jnp.bfloat16)
    own_prob = (own_exp / denominator).astype(jnp.bfloat16).astype(jnp.float32)
    head_owner = owner[:, :head]
    mixed = jnp.zeros((rows, head), jnp.float32)
    for b in range(seqs):
        mixed = jnp.where(head_owner == b, wide_dot(past_prob, values[b]), mixed)
    mixed = mixed + own_prob * jnp.concatenate([new_value] * groups, axis=0)
    heads_out = [mixed[g * seqs : (g + 1) * seqs] for g in range(groups)]
    heads_out = jnp.concatenate(heads_out, axis=1).astype(jnp.bfloat16)
    product = wide_dot(heads_out, out_weight[...]).astype(jnp.bfloat16)
    for peer in range(partial.shape[0]):
        partial[peer] = product
    for copy in copies:
        copy.wait()


def rows_kernel(member, partial, tokens, ffn_gain, notes, residual, outgoing):
    attended = jnp.sum(partial[...].astype(jnp.float32), axis=0)
    full = tokens[...].astype(jnp.float32) + attended
    residual[...] = full
    normed = scaled(full, ffn_gain[...].astype(jnp.float32))
    normed = normed.astype(jnp.bfloat16).astype(jnp.float32)
    marks = notes[...]
    members = full.shape[0] // 2
    here = lax.broadcasted_iota(jnp.int32, (members, 1), 0) == member[0]
    pieces = []
    for half in range(2):
        rows = slice(half * members, (half + 1) * members)
        row = jnp.sum(jnp.where(here, normed[rows], 0.0), axis=0, keepdims=True)
        mark = jnp.sum(jnp.where(here, marks[rows], 0.0), axis=0, keepdims=True)
        pieces += [row[:, k : k + LANES] for k in range(0, full.shape[1], LANES)]
        pieces += [mark, jnp.zeros_like(mark)]
    pattern = jnp.concatenate(pieces * 4, axis=0).astype(jnp.bfloat16)
    step = pattern.shape[0]
    for i in range(outgoing.shape[0] // step):
        outgoing[i * step : (i + 1) * step, :] = pattern


def share_kernel(place, rows, front, pair_front, *refs):
    packs, (out, wide, narrow, columns) = refs[:-4], refs[-4:]
    members = len(packs) // 2
    width = front.shape[1]
    count = narrow.shape[0]
    blocks = width // LANES
    stride = blocks + NOTE_ROWS
    wide[...] = rows[...].astype(jnp.float32)
    for k in range(blocks):
        piece = wide[pl.ds(k, count, stride=stride), :]
        narrow[:, k * LANES : (k + 1) * LANES] = piece.astype(jnp.bfloat16)
    marks = wide[pl.ds(blocks, count, stride=stride), :]
    values = narrow[...]
    down_start = 2 * width
    shared_start = down_start + blocks * LANES
    per_member = blocks // members
    units = (packs[0].shape[0] - shared_start) // per_member

    fronts = [
        lax.dot_general(
            values, each[...], (((1,), (1,)), ((), ())), preferred_element_type=jnp.float32
        )
        for each in (front, pair_front)
    ]
    mix_gate = 1.0 / (1.0 + jnp.exp(-fronts[0][:, 2 * units : 2 * units + 1]))
    shared = [silu(pre[:, :units]) * pre[:, units : 2 * units] for pre in fronts]
    shared = [each.astype(jnp.bfloat16) for each in shared]
    for s in range(members):
        for k in range(per_member):
            rows_of = pl.ds(shared_start + k * units, units)
            dense = wide_dot(shared[0], packs[s][rows_of, :])
            dense = dense + wide_dot(shared[1], packs[members + s][rows_of, :])
            columns[place[2 + s] + k] = mix_gate * dense

    hidden = []
    for side in range(2):
        me = place[side].astype(jnp.float32)
        weight = jnp.zeros((count, 1), jnp.float32)
        for j in range(2):
            chosen = marks[:, j : j + 1] == me
            norm_weight = marks[:, 2 + j : 3 + j] + marks[:, 4 + j : 5 + j]
            weight = weight + jnp.where(chosen, norm_weight, 0.0)
        for s in range(members):
            pack = packs[side * members + s]
            gate = wide_dot(values, pack[:width, :])
            up = wide_dot(values, pack[width : 2 * width, :])
            hidden.append((weight, (silu(gate) * up).astype(jnp.bfloat16)))
    for k in range(blocks):
        total = columns[k]
        for side in range(2):
            first = down_start + k * LANES
            routed = jnp.zeros((count, LANES), jnp.float32)
            for s in range(members):
                weight, each = hidden[side * members + s]
                pack = packs[side * members + s]
                routed = routed + wide_dot(each, pack[first : first + LANES, :])
            total = total + weight * routed
        wide[pl.ds(k, count, stride=blocks), :] = total
    out[...] = wide[: count * blocks, :].astype(jnp.bfloat16)


def per_device(
    tokens,
    lengths,
    cache_keys,
    cache_values,
    cache_cum,
    norm_gain,
    query_weight,
    key_weight,
    value_weight,
    forget_weight,
    forget_bias,
    query_gain,
    key_gain,
    out_weight,
    ffn_gain,
    mix_weight,
    shared_gate,
    shared_up,
    shared_down,
    routes,
    route_weights,
    expert_gate,
    expert_up,
    expert_down,
):
    seqs, width = tokens.shape
    cache_len, head = cache_keys.shape[1], cache_keys.shape[3]
    peers = lax.axis_size(EP)
    members = lax.axis_size("tp")
    member = lax.axis_index("tp")
    blocks = width // LANES
    units = shared_gate.shape[1]
    hidden = expert_gate.shape[2]
    pack_rows = 2 * width + hidden * blocks + units * shared_down.shape[1] // LANES
    copies = 2 + blocks + shared_down.shape[1] // LANES

    partial, packed = pl.pallas_call(
        attend_kernel,
        in_specs=[SMEM, SMEM] + [VMEM] * 12 + [ANY] * 4,
        out_specs=[VMEM, ANY],
        out_shape=[
            jax.ShapeDtypeStruct((members, seqs, width), jnp.bfloat16),
            jax.ShapeDtypeStruct((pack_rows, LANES), jnp.bfloat16),
        ],
        scratch_shapes=[pltpu.SemaphoreType.DMA((copies,))],
        name="attend",
    )(
        lengths,
        forget_bias,
        tokens,
        cache_keys.reshape(seqs, cache_len, head),
        cache_values.reshape(seqs, cache_len, head),
        cache_cum,
        norm_gain[None],
        query_weight,
        key_weight,
        value_weight,
        forget_weight.reshape(1, width),
        query_gain[None],
        key_gain[None],
        out_weight,
        expert_gate[0],
        expert_up[0],
        expert_down[0],
        shared_down,
    )
    partial = lax.all_to_all(partial, "tp", 0, 0, tiled=True)
    packs = [packed]
    for step in (1, members - 1, *range(2, members - 1)):
        ring = [(i, (i + step) % members) for i in range(members)]
        packs.append(lax.ppermute(packed, "tp", ring))

    norm_weights = route_weights / jnp.sum(route_weights, axis=1, keepdims=True)
    high = norm_weights.astype(jnp.bfloat16).astype(jnp.float32)
    low = norm_weights - high
    notes = jnp.concatenate([routes.astype(jnp.float32), high, low], axis=1)
    notes = jnp.pad(notes, ((0, 0), (0, LANES - notes.shape[1])))
    front = [shared_gate.T, shared_up.T, mix_weight[None]]
    front = jnp.concatenate(front, axis=0)
    front = jnp.pad(front, ((0, LANES - front.shape[0]), (0, 0)))
    chip = (lax.axis_index(EP) // 2).astype(jnp.int32)
    core = lax.axis_index(PAIR).astype(jnp.int32)
    steps = jnp.array([0, 1, members - 1, *range(2, members - 1)], jnp.int32)
    origins = (member.astype(jnp.int32) - steps) % members
    place = [2 * chip + core, 2 * chip + 1 - core]
    place += [origins[i] * (blocks // members) for i in range(members)]
    place = jnp.stack(place)

    sub_rows = peers * (blocks + NOTE_ROWS)
    residual, outgoing = pl.pallas_call(
        rows_kernel,
        in_specs=[SMEM] + [VMEM] * 4,
        out_specs=[VMEM, VMEM],
        out_shape=[
            jax.ShapeDtypeStruct((seqs, width), jnp.float32),
            jax.ShapeDtypeStruct((sub_rows, LANES), jnp.bfloat16),
        ],
        name="rows",
    )(member.astype(jnp.int32).reshape(1), partial, tokens, ffn_gain[None], notes)
    own_rows = lax.all_to_all(outgoing.reshape(-1, 2, LANES), EP, 0, 0, tiled=True)

    pair_front = swap(front)
    pair_packs = []
    for pack in packs:
        pair_packs.append(swap(pack))
    total = pl.pallas_call(
        share_kernel,
        in_specs=[SMEM] + [VMEM] * (3 + 2 * members),
        out_specs=VMEM,
        out_shape=jax.ShapeDtypeStruct((peers * blocks, LANES), jnp.bfloat16),
        scratch_shapes=[
            pltpu.VMEM((sub_rows, LANES), jnp.float32),
            pltpu.VMEM((peers, width), jnp.bfloat16),
            pltpu.VMEM((blocks, peers, LANES), jnp.float32),
        ],
        name="share",
    )(place, own_rows.reshape(sub_rows, LANES), front, pair_front, *packs, *pair_packs)
    returned = lax.all_to_all(total.reshape(-1, 2, LANES), (*EP, "tp"), 0, 0, tiled=True)
    returned = returned.reshape(peers // 2, seqs, -1, LANES).astype(jnp.float32)
    returned = jnp.sum(returned, axis=0).reshape(seqs, -1)
    slice_width = returned.shape[1]
    residual_slice = lax.dynamic_slice_in_dim(residual, member * slice_width, slice_width, 1)
    return (residual_slice + returned).astype(jnp.bfloat16)


def solution(mesh):
    finer = Mesh(mesh.devices.reshape(16, 4, 2, mesh.shape["tp"]), ("ep_0", "ep_1", "ep_2", "tp"))
    placed = (
        P(EP, None),
        P(EP),
        P(EP, None, "tp", None),
        P(EP, None, "tp", None),
        P(EP, "tp", None),
        P(),
        P(None, "tp"),
        P(None, "tp"),
        P(None, "tp"),
        P(None, "tp"),
        P("tp"),
        P(),
        P(),
        P("tp", None),
        P(),
        P(),
        P(None, EP),
        P(None, EP),
        P(EP, "tp"),
        P(EP, None),
        P(EP, None),
        P(EP, None, "tp"),
        P(EP, None, "tp"),
        P(EP, "tp", None),
    )

    return jax.shard_map(
        per_device, mesh=finer, in_specs=placed, out_specs=P(EP, "tp"), check_vma=False
    )
```

```python
import jax
import jax.numpy as jnp
from jax import lax
from jax.experimental import pallas as pl
from jax.experimental.pallas import tpu as pltpu
from jax.sharding import Mesh
from jax.sharding import PartitionSpec as P

EP = ("ep_0", "ep_1", "ep_2")
PAIR = "ep_2"
LANES = 128
NOTE_ROWS = 2

epsilon = 1e-06

VMEM = pl.BlockSpec(memory_space=pltpu.VMEM)
SMEM = pl.BlockSpec(memory_space=pltpu.SMEM)
ANY = pl.BlockSpec(memory_space=pl.ANY)


def swap(shard):
    return lax.ppermute(shard, PAIR, [(0, 1), (1, 0)])


def scaled(values, gain):
    mean = jnp.mean(values * values, axis=-1, keepdims=True)
    return values * lax.rsqrt(mean + epsilon) * gain


def silu(values):
    return values / (1.0 + jnp.exp(-values))


def in_vmem(values):
    return pltpu.with_memory_space_constraint(values, pltpu.VMEM)


def ring_steps(members):
    return (0, 1, members - 1, *range(2, members - 1))


def wide_dot(left, right):
    return jnp.dot(left, right, preferred_element_type=jnp.float32)


def attend_kernel(
    lengths,
    forget_bias,
    norm_gain,
    query_gain,
    key_gain,
    forget_weight,
    tokens_hbm,
    query_weight_hbm,
    key_weight_hbm,
    value_weight_hbm,
    cum_hbm,
    keys_hbm,
    values_hbm,
    out_weight_hbm,
    expert_gate,
    expert_up,
    expert_down,
    shared_down,
    partial,
    packed,
    tokens,
    query_weight,
    key_weight,
    value_weight,
    cum,
    keys,
    values,
    out_weight,
    sems,
):
    copies = []

    def start(source, target):
        copy = pltpu.make_async_copy(source, target, sems.at[len(copies)])
        copy.start()
        copies.append(copy)
        return copy

    tokens_in = start(tokens_hbm, tokens)
    query_in = start(query_weight_hbm, query_weight)
    key_in = start(key_weight_hbm, key_weight)
    value_in = start(value_weight_hbm, value_weight)
    keys_in = start(keys_hbm, keys)
    cum_in = start(cum_hbm, cum)
    values_in = start(values_hbm, values)
    out_in = start(out_weight_hbm, out_weight)
    first_packed = len(copies)
    row = 0

    def pack(source, row):
        start(source, packed.at[pl.ds(row, source.shape[0]), :])
        return row + source.shape[0]

    row = pack(expert_gate, row)
    row = pack(expert_up, row)
    for block in range(expert_down.shape[1] // LANES):
        row = pack(expert_down.at[:, pl.ds(block * LANES, LANES)], row)
    for block in range(shared_down.shape[1] // LANES):
        row = pack(shared_down.at[:, pl.ds(block * LANES, LANES)], row)

    seqs, cache_len, head = keys.shape
    groups = query_weight.shape[1] // head
    tokens_in.wait()
    normed = scaled(tokens[...].astype(jnp.float32), norm_gain[...].astype(jnp.float32))
    normed = normed.astype(jnp.bfloat16)
    gain = query_gain[...].astype(jnp.float32)
    query_in.wait()
    wide = wide_dot(normed, query_weight[...])
    query = [scaled(wide[:, g * head : (g + 1) * head], gain) for g in range(groups)]
    query = jnp.concatenate(query, axis=0).astype(jnp.bfloat16)
    key_in.wait()
    new_key = scaled(wide_dot(normed, key_weight[...]), key_gain[...].astype(jnp.float32))
    new_key = new_key.astype(jnp.bfloat16).astype(jnp.float32)
    value_in.wait()
    new_value = wide_dot(normed, value_weight[...]).astype(jnp.bfloat16).astype(jnp.float32)
    products = normed.astype(jnp.float32) * forget_weight[...].astype(jnp.float32)
    forget = jnp.sum(products, axis=-1, keepdims=True) + forget_bias[0]
    new_log = jnp.minimum(forget, 0.0) - jnp.log1p(jnp.exp(-jnp.abs(forget)))

    rows = groups * seqs
    owner = lax.broadcasted_iota(jnp.int32, (rows, cache_len), 0) % seqs
    position = lax.broadcasted_iota(jnp.int32, (rows, cache_len), 1)
    scores = jnp.zeros((rows, cache_len), jnp.float32)
    decay = jnp.zeros((rows, cache_len), jnp.float32)
    length = jnp.zeros((rows, cache_len), jnp.int32)
    keys_in.wait()
    cum_in.wait()
    for b in range(seqs):
        mine = owner == b
        one = lax.dot_general(
            query, keys[b], (((1,), (1,)), ((), ())), preferred_element_type=jnp.float32
        )
        scores = jnp.where(mine, one, scores)
        decay = jnp.where(mine, cum[b], decay)
        length = jnp.where(mine, lengths[b], length)
    last = jnp.where(position == length - 1, decay, 0.0)
    last = jnp.sum(last, axis=-1, keepdims=True)
    bias = last - decay + jnp.concatenate([new_log] * groups, axis=0)
    score_scale = head ** (-0.5)
    past = jnp.where(position < length, scores * score_scale + bias, -jnp.inf)
    own = query.astype(jnp.float32) * jnp.concatenate([new_key] * groups, axis=0)
    own = jnp.sum(own, axis=-1, keepdims=True) * score_scale
    past_exp = jnp.exp(past)
    own_exp = jnp.exp(own)
    denominator = jnp.sum(past_exp, axis=-1, keepdims=True) + own_exp
    past_prob = (past_exp / denominator).astype(jnp.bfloat16)
    own_prob = (own_exp / denominator).astype(jnp.bfloat16).astype(jnp.float32)
    head_owner = owner[:, :head]
    mixed = jnp.zeros((rows, head), jnp.float32)
    values_in.wait()
    for b in range(seqs):
        mixed = jnp.where(head_owner == b, wide_dot(past_prob, values[b]), mixed)
    mixed = mixed + own_prob * jnp.concatenate([new_value] * groups, axis=0)
    heads_out = [mixed[g * seqs : (g + 1) * seqs] for g in range(groups)]
    heads_out = jnp.concatenate(heads_out, axis=1).astype(jnp.bfloat16)
    out_in.wait()
    product = wide_dot(heads_out, out_weight[...]).astype(jnp.bfloat16)
    for peer in range(partial.shape[0]):
        partial[peer] = product
    for copy in copies[first_packed:]:
        copy.wait()


def rows_kernel(partial, tokens, ffn_gain, routes, route_weights, residual, outgoing):
    member = lax.axis_index("tp")
    attended = jnp.sum(partial[...].astype(jnp.float32), axis=0)
    full = tokens[...].astype(jnp.float32) + attended
    seqs, width = full.shape
    members = partial.shape[0]
    slice_width = width // members
    for t in range(members):

        @pl.when(member == t)
        def _():
            residual[...] = full[:, t * slice_width : (t + 1) * slice_width]

    normed = scaled(full, ffn_gain[...].astype(jnp.float32))
    normed = normed.astype(jnp.bfloat16).astype(jnp.float32)
    norm_weights = route_weights[...]
    norm_weights = norm_weights / jnp.sum(norm_weights, axis=0, keepdims=True)
    high = norm_weights.astype(jnp.bfloat16).astype(jnp.float32)
    low = norm_weights - high
    marks = (routes[...].astype(jnp.float32), high, low)
    column = lax.broadcasted_iota(jnp.int32, routes.shape, 1)
    lane = lax.broadcasted_iota(jnp.int32, (1, LANES), 1)
    rows_here = lax.broadcasted_iota(jnp.int32, (seqs, width), 0)
    pieces = []
    for half in range(2):
        at = half * members + member
        row = jnp.sum(jnp.where(rows_here == at, normed, 0.0), axis=0, keepdims=True)
        mark = jnp.zeros((1, LANES), jnp.float32)
        for i, values in enumerate(marks):
            here = jnp.sum(jnp.where(column == at, values, 0.0), axis=1, keepdims=True)
            for j in range(2):
                mark = jnp.where(lane == 2 * i + j, here[j : j + 1], mark)
        pieces += [row[:, k : k + LANES] for k in range(0, width, LANES)]
        pieces += [mark, jnp.zeros_like(mark)]
    pattern = jnp.concatenate(pieces * 4, axis=0).astype(jnp.bfloat16)
    step = pattern.shape[0]
    for i in range(outgoing.shape[0] // step):
        outgoing[i * step : (i + 1) * step, :] = pattern


def share_kernel(rows, front, pair_front, *refs):
    sources, (out, wide, narrow, columns, staged, sems) = refs[:-6], refs[-6:]
    members = len(sources) // 2
    packs, arrivals = [sources[0]], [None]
    for i, source in enumerate(sources[1:]):
        copy = pltpu.make_async_copy(source, staged.at[i], sems.at[i])
        copy.start()
        packs.append(staged.at[i])
        arrivals.append(copy)
    member = lax.axis_index("tp")
    core = lax.axis_index(PAIR)
    experts = (lax.axis_index(EP), lax.axis_index(EP) + 1 - 2 * core)
    width = front.shape[1]
    count = narrow.shape[0]
    blocks = width // LANES
    stride = blocks + NOTE_ROWS
    wide[...] = rows[...].astype(jnp.float32)
    for k in range(blocks):
        piece = wide[pl.ds(k, count, stride=stride), :]
        narrow[:, k * LANES : (k + 1) * LANES] = piece.astype(jnp.bfloat16)
    marks = wide[pl.ds(blocks, count, stride=stride), :]
    values = narrow[...]
    down_start = 2 * width
    shared_start = down_start + blocks * LANES
    per_member = blocks // members
    units = (packs[0].shape[0] - shared_start) // per_member

    fronts = [
        lax.dot_general(
            values, each[...], (((1,), (1,)), ((), ())), preferred_element_type=jnp.float32
        )
        for each in (front, pair_front)
    ]
    mix_gate = 1.0 / (1.0 + jnp.exp(-fronts[0][:, 2 * units : 2 * units + 1]))
    hidden = []
    for side in range(2):
        me = experts[side].astype(jnp.float32)
        weight = jnp.zeros((count, 1), jnp.float32)
        for j in range(2):
            chosen = marks[:, j : j + 1] == me
            norm_weight = marks[:, 2 + j : 3 + j] + marks[:, 4 + j : 5 + j]
            weight = weight + jnp.where(chosen, norm_weight, 0.0)
        for s in range(members):
            pack = packs[side * members + s]
            if arrivals[side * members + s] is not None:
                arrivals[side * members + s].wait()
            gate = wide_dot(values, pack[:width, :])
            up = wide_dot(values, pack[width : 2 * width, :])
            hidden.append((weight, (silu(gate) * up).astype(jnp.bfloat16)))
    shared = [silu(pre[:, :units]) * pre[:, units : 2 * units] for pre in fronts]
    shared = [each.astype(jnp.bfloat16) for each in shared]
    for s, step in enumerate(ring_steps(members)):
        origin = (member + members - step) % members
        for k in range(per_member):
            rows_of = pl.ds(shared_start + k * units, units)
            dense = wide_dot(shared[0], packs[s][rows_of, :])
            dense = dense + wide_dot(shared[1], packs[members + s][rows_of, :])
            columns[origin * per_member + k] = mix_gate * dense

    for k in range(blocks):
        total = columns[k]
        for side in range(2):
            first = down_start + k * LANES
            routed = jnp.zeros((count, LANES), jnp.float32)
            for s in range(members):
                weight, each = hidden[side * members + s]
                pack = packs[side * members + s]
                routed = routed + wide_dot(each, pack[first : first + LANES, :])
            total = total + weight * routed
        wide[pl.ds(k, count, stride=blocks), :] = total
    out[...] = wide[: count * blocks, :].astype(jnp.bfloat16)


def per_device(
    tokens,
    lengths,
    cache_keys,
    cache_values,
    cache_cum,
    norm_gain,
    query_weight,
    key_weight,
    value_weight,
    forget_weight,
    forget_bias,
    query_gain,
    key_gain,
    out_weight,
    ffn_gain,
    mix_weight,
    shared_gate,
    shared_up,
    shared_down,
    routes,
    route_weights,
    expert_gate,
    expert_up,
    expert_down,
):
    seqs, width = tokens.shape
    cache_len, head = cache_keys.shape[1], cache_keys.shape[3]
    peers = lax.axis_size(EP)
    members = lax.axis_size("tp")
    blocks = width // LANES
    units = shared_gate.shape[1]
    hidden = expert_gate.shape[2]
    pack_rows = 2 * width + hidden * blocks + units * shared_down.shape[1] // LANES
    copies = 2 + blocks + shared_down.shape[1] // LANES

    big = [
        tokens,
        query_weight,
        key_weight,
        value_weight,
        cache_cum,
        cache_keys.reshape(seqs, cache_len, head),
        cache_values.reshape(seqs, cache_len, head),
        out_weight,
    ]
    partial, packed = pl.pallas_call(
        attend_kernel,
        in_specs=[SMEM, SMEM] + [VMEM] * 4 + [ANY] * (len(big) + 4),
        out_specs=[VMEM, VMEM],
        out_shape=[
            pltpu.VMEM((members, seqs, width), jnp.bfloat16),
            pltpu.VMEM((pack_rows, LANES), jnp.bfloat16),
        ],
        scratch_shapes=[pltpu.VMEM(each.shape, each.dtype) for each in big]
        + [pltpu.SemaphoreType.DMA((copies + len(big),))],
        name="attend",
    )(
        lengths,
        forget_bias,
        norm_gain,
        query_gain,
        key_gain,
        forget_weight.reshape(1, width),
        *big,
        expert_gate[0],
        expert_up[0],
        expert_down[0],
        shared_down,
    )
    partial = lax.all_to_all(partial, "tp", 0, 0, tiled=True)
    packs = [packed]
    for step in ring_steps(members)[1:]:
        ring = [(i, (i + step) % members) for i in range(members)]
        packs.append(lax.ppermute(packed, "tp", ring))

    front = [shared_gate.T, shared_up.T, mix_weight[None]]
    front = jnp.concatenate(front, axis=0)
    front = jnp.pad(front, ((0, LANES - front.shape[0]), (0, 0)))

    sub_rows = peers * (blocks + NOTE_ROWS)
    residual, outgoing = pl.pallas_call(
        rows_kernel,
        in_specs=[VMEM] * 5,
        out_specs=[VMEM, VMEM],
        out_shape=[
            jax.ShapeDtypeStruct((seqs, width // members), jnp.float32),
            pltpu.VMEM((sub_rows, LANES), jnp.bfloat16),
        ],
        name="rows",
    )(in_vmem(partial), tokens, ffn_gain, routes.T, route_weights.T)
    own_rows = lax.all_to_all(outgoing.reshape(-1, 2, LANES), EP, 0, 0, tiled=True)

    pair_front = swap(front)
    pair_packs = []
    for pack in packs:
        pair_packs.append(swap(pack))
    total = pl.pallas_call(
        share_kernel,
        in_specs=[VMEM] * 4 + [ANY] * (2 * members - 1),
        out_specs=VMEM,
        out_shape=pltpu.VMEM((peers * blocks, LANES), jnp.bfloat16),
        scratch_shapes=[
            pltpu.VMEM((sub_rows, LANES), jnp.float32),
            pltpu.VMEM((peers, width), jnp.bfloat16),
            pltpu.VMEM((blocks, peers, LANES), jnp.float32),
            pltpu.VMEM((2 * members - 1, pack_rows, LANES), jnp.bfloat16),
            pltpu.SemaphoreType.DMA((2 * members - 1,)),
        ],
        name="share",
    )(
        *map(in_vmem, (own_rows.reshape(sub_rows, LANES), front, pair_front, packed)),
        *packs[1:],
        *pair_packs,
    )
    returned = lax.all_to_all(total.reshape(-1, 2, LANES), (*EP, "tp"), 0, 0, tiled=True)
    returned = returned.reshape(peers // 2, seqs, -1, LANES).astype(jnp.float32)
    returned = jnp.sum(returned, axis=0).reshape(seqs, -1)
    return (residual + returned).astype(jnp.bfloat16)


def solution(mesh):
    finer = Mesh(mesh.devices.reshape(16, 4, 2, mesh.shape["tp"]), ("ep_0", "ep_1", "ep_2", "tp"))
    placed = (
        P(EP, None),
        P(EP),
        P(EP, None, "tp", None),
        P(EP, None, "tp", None),
        P(EP, "tp", None),
        P(),
        P(None, "tp"),
        P(None, "tp"),
        P(None, "tp"),
        P(None, "tp"),
        P("tp"),
        P(),
        P(),
        P("tp", None),
        P(),
        P(),
        P(None, EP),
        P(None, EP),
        P(EP, "tp"),
        P(EP, None),
        P(EP, None),
        P(EP, None, "tp"),
        P(EP, None, "tp"),
        P(EP, "tp", None),
    )

    return jax.shard_map(
        per_device, mesh=finer, in_specs=placed, out_specs=P(EP, "tp"), check_vma=False
    )
```

```python
import jax
import jax.numpy as jnp
from jax import lax
from jax.experimental import pallas as pl
from jax.experimental.pallas import tpu as pltpu
from jax.sharding import Mesh
from jax.sharding import PartitionSpec as P

EP = ("ep_0", "ep_1", "ep_2")
PAIR = "ep_2"
LANES = 128
NOTE_ROWS = 2

epsilon = 1e-06

VMEM = pl.BlockSpec(memory_space=pltpu.VMEM)
SMEM = pl.BlockSpec(memory_space=pltpu.SMEM)
ANY = pl.BlockSpec(memory_space=pl.ANY)


def swap(shard):
    return lax.ppermute(shard, PAIR, [(0, 1), (1, 0)])


def scaled(values, gain):
    mean = jnp.mean(values * values, axis=-1, keepdims=True)
    return values * lax.rsqrt(mean + epsilon) * gain


def silu(values):
    return values / (1.0 + jnp.exp(-values))


def in_vmem(values):
    return pltpu.with_memory_space_constraint(values, pltpu.VMEM)


def shifted(shard, step, members):
    pairs = []
    for core, sign in enumerate((1, -1)):
        for t in range(members):
            target = (t + sign * step) % members
            pairs.append((core * members + t, core * members + target))
    return lax.ppermute(shard, (PAIR, "tp"), pairs)


def wide_dot(left, right):
    return jnp.dot(left, right, preferred_element_type=jnp.float32)


def attend_kernel(
    lengths,
    forget_bias,
    norm_gain,
    query_gain,
    key_gain,
    forget_weight,
    tokens_hbm,
    query_weight_hbm,
    key_weight_hbm,
    value_weight_hbm,
    cum_hbm,
    keys_hbm,
    values_hbm,
    out_weight_hbm,
    expert_gate,
    expert_up,
    expert_down,
    shared_down,
    partial,
    packed,
    tokens,
    query_weight,
    key_weight,
    value_weight,
    cum,
    keys,
    values,
    out_weight,
    sems,
):
    copies = []

    def start(source, target):
        copy = pltpu.make_async_copy(source, target, sems.at[len(copies)])
        copy.start()
        copies.append(copy)
        return copy

    tokens_in = start(tokens_hbm, tokens)
    query_in = start(query_weight_hbm, query_weight)
    key_in = start(key_weight_hbm, key_weight)
    value_in = start(value_weight_hbm, value_weight)
    keys_in = start(keys_hbm, keys)
    cum_in = start(cum_hbm, cum)
    values_in = start(values_hbm, values)
    out_in = start(out_weight_hbm, out_weight)
    first_packed = len(copies)
    row = 0

    def pack(source, row):
        start(source, packed.at[pl.ds(row, source.shape[0]), :])
        return row + source.shape[0]

    row = pack(expert_gate, row)
    row = pack(expert_up, row)
    for block in range(expert_down.shape[1] // LANES):
        row = pack(expert_down.at[:, pl.ds(block * LANES, LANES)], row)
    for block in range(shared_down.shape[1] // LANES):
        row = pack(shared_down.at[:, pl.ds(block * LANES, LANES)], row)

    seqs, cache_len, head = keys.shape
    groups = query_weight.shape[1] // head
    tokens_in.wait()
    normed = scaled(tokens[...].astype(jnp.float32), norm_gain[...].astype(jnp.float32))
    normed = normed.astype(jnp.bfloat16)
    gain = query_gain[...].astype(jnp.float32)
    query_in.wait()
    wide = wide_dot(normed, query_weight[...])
    query = [scaled(wide[:, g * head : (g + 1) * head], gain) for g in range(groups)]
    query = jnp.concatenate(query, axis=0).astype(jnp.bfloat16)
    key_in.wait()
    new_key = scaled(wide_dot(normed, key_weight[...]), key_gain[...].astype(jnp.float32))
    new_key = new_key.astype(jnp.bfloat16).astype(jnp.float32)
    value_in.wait()
    new_value = wide_dot(normed, value_weight[...]).astype(jnp.bfloat16).astype(jnp.float32)
    products = normed.astype(jnp.float32) * forget_weight[...].astype(jnp.float32)
    forget = jnp.sum(products, axis=-1, keepdims=True) + forget_bias[0]
    new_log = jnp.minimum(forget, 0.0) - jnp.log1p(jnp.exp(-jnp.abs(forget)))

    rows = groups * seqs
    owner = lax.broadcasted_iota(jnp.int32, (rows, cache_len), 0) % seqs
    position = lax.broadcasted_iota(jnp.int32, (rows, cache_len), 1)
    scores = jnp.zeros((rows, cache_len), jnp.float32)
    decay = jnp.zeros((rows, cache_len), jnp.float32)
    length = jnp.zeros((rows, cache_len), jnp.int32)
    keys_in.wait()
    cum_in.wait()
    for b in range(seqs):
        mine = owner == b
        one = lax.dot_general(
            query, keys[b], (((1,), (1,)), ((), ())), preferred_element_type=jnp.float32
        )
        scores = jnp.where(mine, one, scores)
        decay = jnp.where(mine, cum[b], decay)
        length = jnp.where(mine, lengths[b], length)
    last = jnp.where(position == length - 1, decay, 0.0)
    last = jnp.sum(last, axis=-1, keepdims=True)
    bias = last - decay + jnp.concatenate([new_log] * groups, axis=0)
    score_scale = head ** (-0.5)
    past = jnp.where(position < length, scores * score_scale + bias, -jnp.inf)
    own = query.astype(jnp.float32) * jnp.concatenate([new_key] * groups, axis=0)
    own = jnp.sum(own, axis=-1, keepdims=True) * score_scale
    past_exp = jnp.exp(past)
    own_exp = jnp.exp(own)
    denominator = jnp.sum(past_exp, axis=-1, keepdims=True) + own_exp
    past_prob = (past_exp / denominator).astype(jnp.bfloat16)
    own_prob = (own_exp / denominator).astype(jnp.bfloat16).astype(jnp.float32)
    head_owner = owner[:, :head]
    mixed = jnp.zeros((rows, head), jnp.float32)
    values_in.wait()
    for b in range(seqs):
        mixed = jnp.where(head_owner == b, wide_dot(past_prob, values[b]), mixed)
    mixed = mixed + own_prob * jnp.concatenate([new_value] * groups, axis=0)
    heads_out = [mixed[g * seqs : (g + 1) * seqs] for g in range(groups)]
    heads_out = jnp.concatenate(heads_out, axis=1).astype(jnp.bfloat16)
    out_in.wait()
    product = wide_dot(heads_out, out_weight[...]).astype(jnp.bfloat16)
    for peer in range(partial.shape[0]):
        partial[peer] = product
    for copy in copies[first_packed:]:
        copy.wait()


def rows_kernel(partial, tokens, ffn_gain, routes, route_weights, residual, outgoing):
    member = lax.axis_index("tp")
    attended = jnp.sum(partial[...].astype(jnp.float32), axis=0)
    full = tokens[...].astype(jnp.float32) + attended
    seqs, width = full.shape
    members = partial.shape[0]
    slice_width = width // members
    for t in range(members):

        @pl.when(member == t)
        def _():
            residual[...] = full[:, t * slice_width : (t + 1) * slice_width]

    normed = scaled(full, ffn_gain[...].astype(jnp.float32))
    normed = normed.astype(jnp.bfloat16).astype(jnp.float32)
    norm_weights = route_weights[...]
    norm_weights = norm_weights / jnp.sum(norm_weights, axis=0, keepdims=True)
    high = norm_weights.astype(jnp.bfloat16).astype(jnp.float32)
    low = norm_weights - high
    marks = (routes[...].astype(jnp.float32), high, low)
    column = lax.broadcasted_iota(jnp.int32, routes.shape, 1)
    lane = lax.broadcasted_iota(jnp.int32, (1, LANES), 1)
    rows_here = lax.broadcasted_iota(jnp.int32, (seqs, width), 0)
    pieces = []
    for half in range(2):
        at = half * members + member
        row = jnp.sum(jnp.where(rows_here == at, normed, 0.0), axis=0, keepdims=True)
        mark = jnp.zeros((1, LANES), jnp.float32)
        for i, values in enumerate(marks):
            here = jnp.sum(jnp.where(column == at, values, 0.0), axis=1, keepdims=True)
            for j in range(2):
                mark = jnp.where(lane == 2 * i + j, here[j : j + 1], mark)
        pieces += [row[:, k : k + LANES] for k in range(0, width, LANES)]
        pieces += [mark, jnp.zeros_like(mark)]
    pattern = jnp.concatenate(pieces * 4, axis=0).astype(jnp.bfloat16)
    step = pattern.shape[0]
    for i in range(outgoing.shape[0] // step):
        outgoing[i * step : (i + 1) * step, :] = pattern


def share_kernel(rows, front, pair_front, packed, *refs):
    sources, (out, wide, narrow, columns, staged, sems) = refs[:-6], refs[-6:]
    copies = []
    for i, source in enumerate(sources):
        copies.append(pltpu.make_async_copy(source, staged.at[i], sems.at[i]))
        copies[-1].start()
    packs = [packed] + [staged.at[i] for i in range(len(sources))]
    members = len(packs) // 2
    member = lax.axis_index("tp")
    core = lax.axis_index(PAIR)
    experts = (lax.axis_index(EP), lax.axis_index(EP) + 1 - 2 * core)
    width = front.shape[1]
    count = narrow.shape[0]
    blocks = width // LANES
    stride = blocks + NOTE_ROWS
    lines = lax.axis_size("ep_1") * 2
    depth = count // lines
    wide[...] = rows[...].astype(jnp.float32)
    marks = []
    for line in range(lines):
        for k in range(blocks + 1):
            piece = wide[pl.ds(line * stride + k, depth, stride=lines * stride), :]
            if k < blocks:
                at = (slice(line * depth, (line + 1) * depth), slice(k * LANES, (k + 1) * LANES))
                narrow[at] = piece.astype(jnp.bfloat16)
            else:
                marks.append(piece)
    marks = jnp.concatenate(marks, axis=0)
    values = narrow[...]
    down_start = 2 * width
    shared_start = down_start + blocks * LANES
    per_member = blocks // members
    units = (packs[0].shape[0] - shared_start) // per_member

    fronts = [
        lax.dot_general(
            values, each[...], (((1,), (1,)), ((), ())), preferred_element_type=jnp.float32
        )
        for each in (front, pair_front)
    ]
    mix_gate = 1.0 / (1.0 + jnp.exp(-fronts[0][:, 2 * units : 2 * units + 1]))
    hidden = []
    for side in range(2):
        me = experts[side].astype(jnp.float32)
        weight = jnp.zeros((count, 1), jnp.float32)
        for j in range(2):
            chosen = marks[:, j : j + 1] == me
            norm_weight = marks[:, 2 + j : 3 + j] + marks[:, 4 + j : 5 + j]
            weight = weight + jnp.where(chosen, norm_weight, 0.0)
        for s in range(members):
            at = side * members + s
            if at:
                copies[at - 1].wait()
            gate = wide_dot(values, packs[at][:width, :])
            up = wide_dot(values, packs[at][width : 2 * width, :])
            hidden.append((weight, (silu(gate) * up).astype(jnp.bfloat16)))
    shared = [silu(pre[:, :units]) * pre[:, units : 2 * units] for pre in fronts]
    shared = [each.astype(jnp.bfloat16) for each in shared]
    ahead = jnp.where(core == 0, members - 1, 1)
    origins = (0, ahead, members - ahead, 2)
    for s, pair in enumerate((0, 2, 1, 3)):
        origin = (member + origins[s]) % members
        for k in range(per_member):
            rows_of = pl.ds(shared_start + k * units, units)
            dense = wide_dot(shared[0], packs[s][rows_of, :])
            dense = dense + wide_dot(shared[1], packs[members + pair][rows_of, :])
            columns[origin * per_member + k] = mix_gate * dense
    for k in range(blocks):
        total = columns[k]
        for side in range(2):
            first = down_start + k * LANES
            routed = jnp.zeros((count, LANES), jnp.float32)
            for s in range(members):
                weight, each = hidden[side * members + s]
                pack = packs[side * members + s]
                routed = routed + wide_dot(each, pack[first : first + LANES, :])
            total = total + weight * routed
        for line in range(lines):
            first = line // 2 * depth * 2 * blocks + k // per_member * depth * 2 * per_member
            first = first + line % 2 * per_member + k % per_member
            piece = total[line * depth : (line + 1) * depth]
            wide[pl.ds(first, depth, stride=2 * per_member), :] = piece
    out[...] = wide[: count * blocks, :].astype(jnp.bfloat16)


def fold_kernel(parts, out, wide, small):
    sources = lax.axis_size("ep_1")
    members = lax.axis_size("tp")
    rows = parts.shape[0] // sources
    wide[...] = parts[...].astype(jnp.float32)
    total = wide[:rows, :]
    for i in range(1, sources):
        total = total + wide[i * rows : (i + 1) * rows, :]
    wide[:rows, :] = total
    halves = 2
    count = rows // members // halves
    for t in range(members):
        for j in range(halves):
            piece = wide[pl.ds(t * count * halves + j, count, stride=halves), :]
            small[pl.ds(t * halves + j, count, stride=members * halves), :] = piece
    out[...] = small[...].astype(jnp.bfloat16)


def finish_kernel(parts, residual, out, small):
    rows = small.shape[0]
    total = parts[:rows, :].astype(jnp.float32)
    for i in range(1, parts.shape[0] // rows):
        total = total + parts[i * rows : (i + 1) * rows, :].astype(jnp.float32)
    small[...] = total
    seqs = residual.shape[0]
    for j in range(rows // seqs):
        piece = small[pl.ds(j, seqs, stride=rows // seqs), :]
        columns = slice(j * LANES, (j + 1) * LANES)
        out[:, columns] = (residual[:, columns] + piece).astype(jnp.bfloat16)


def per_device(
    tokens,
    lengths,
    cache_keys,
    cache_values,
    cache_cum,
    norm_gain,
    query_weight,
    key_weight,
    value_weight,
    forget_weight,
    forget_bias,
    query_gain,
    key_gain,
    out_weight,
    ffn_gain,
    mix_weight,
    shared_gate,
    shared_up,
    shared_down,
    routes,
    route_weights,
    expert_gate,
    expert_up,
    expert_down,
):
    seqs, width = tokens.shape
    cache_len, head = cache_keys.shape[1], cache_keys.shape[3]
    peers = lax.axis_size(EP)
    members = lax.axis_size("tp")
    blocks = width // LANES
    units = shared_gate.shape[1]
    hidden = expert_gate.shape[2]
    pack_rows = 2 * width + hidden * blocks + units * shared_down.shape[1] // LANES
    copies = 2 + blocks + shared_down.shape[1] // LANES

    big = [
        tokens,
        query_weight,
        key_weight,
        value_weight,
        cache_cum,
        cache_keys.reshape(seqs, cache_len, head),
        cache_values.reshape(seqs, cache_len, head),
        out_weight,
    ]
    partial, packed = pl.pallas_call(
        attend_kernel,
        in_specs=[SMEM, SMEM] + [VMEM] * 4 + [ANY] * (len(big) + 4),
        out_specs=[VMEM, VMEM],
        out_shape=[
            pltpu.VMEM((members, seqs, width), jnp.bfloat16),
            pltpu.VMEM((pack_rows, LANES), jnp.bfloat16),
        ],
        scratch_shapes=[pltpu.VMEM(each.shape, each.dtype) for each in big]
        + [pltpu.SemaphoreType.DMA((copies + len(big),))],
        name="attend",
    )(
        lengths,
        forget_bias,
        norm_gain,
        query_gain,
        key_gain,
        forget_weight.reshape(1, width),
        *big,
        expert_gate[0],
        expert_up[0],
        expert_down[0],
        shared_down,
    )
    partial = lax.all_to_all(partial, "tp", 0, 0, tiled=True)
    ahead = shifted(packed, 1, members)
    behind = shifted(packed, -1, members)
    across = shifted(ahead, 1, members)
    packs = [packed, ahead, behind, across]

    front = [shared_gate.T, shared_up.T, mix_weight[None]]
    front = jnp.concatenate(front, axis=0)
    front = jnp.pad(front, ((0, LANES - front.shape[0]), (0, 0)))

    sub_rows = peers * (blocks + NOTE_ROWS)
    residual, outgoing = pl.pallas_call(
        rows_kernel,
        in_specs=[VMEM] * 5,
        out_specs=[VMEM, VMEM],
        out_shape=[
            pltpu.VMEM((seqs, width // members), jnp.float32),
            pltpu.VMEM((sub_rows, LANES), jnp.bfloat16),
        ],
        name="rows",
    )(*map(in_vmem, (partial, tokens, ffn_gain, routes.T, route_weights.T)))
    own_rows = lax.all_to_all(outgoing.reshape(-1, 2, LANES), EP, 0, 0, tiled=True)

    pair_front = swap(front)
    pair_packs = []
    for pack in packs:
        pair_packs.append(swap(pack))
    total = pl.pallas_call(
        share_kernel,
        in_specs=[VMEM] * 4 + [ANY] * (2 * members - 1),
        out_specs=VMEM,
        out_shape=pltpu.VMEM((peers * blocks, LANES), jnp.bfloat16),
        scratch_shapes=[
            pltpu.VMEM((sub_rows, LANES), jnp.float32),
            pltpu.VMEM((peers, width), jnp.bfloat16),
            pltpu.VMEM((blocks, peers, LANES), jnp.float32),
            pltpu.VMEM((2 * members - 1, pack_rows, LANES), jnp.bfloat16),
            pltpu.SemaphoreType.DMA((2 * members - 1,)),
        ],
        name="share",
    )(
        *map(in_vmem, (own_rows.reshape(sub_rows, LANES), front, pair_front, packed)),
        *packs[1:],
        *pair_packs,
    )
    parts = lax.all_to_all(total.reshape(-1, 2, LANES), ("ep_1", "tp"), 0, 0, tiled=True)
    parts = parts.reshape(-1, LANES)
    rows = parts.shape[0] // lax.axis_size("ep_1")
    parts = pl.pallas_call(
        fold_kernel,
        in_specs=[VMEM],
        out_specs=VMEM,
        out_shape=pltpu.VMEM((rows, LANES), jnp.bfloat16),
        scratch_shapes=[
            pltpu.VMEM(parts.shape, jnp.float32),
            pltpu.VMEM((rows, LANES), jnp.float32),
        ],
        name="fold",
    )(in_vmem(parts))
    parts = lax.all_to_all(parts.reshape(-1, 2, LANES), ("ep_0", PAIR), 0, 0, tiled=True)
    return pl.pallas_call(
        finish_kernel,
        in_specs=[VMEM] * 2,
        out_specs=VMEM,
        out_shape=jax.ShapeDtypeStruct((seqs, width // members), jnp.bfloat16),
        scratch_shapes=[pltpu.VMEM((seqs * width // members // LANES, LANES), jnp.float32)],
        name="finish",
    )(in_vmem(parts.reshape(-1, LANES)), in_vmem(residual))


def solution(mesh):
    finer = Mesh(mesh.devices.reshape(16, 4, 2, mesh.shape["tp"]), ("ep_0", "ep_1", "ep_2", "tp"))
    placed = (
        P(EP, None),
        P(EP),
        P(EP, None, "tp", None),
        P(EP, None, "tp", None),
        P(EP, "tp", None),
        P(),
        P(None, "tp"),
        P(None, "tp"),
        P(None, "tp"),
        P(None, "tp"),
        P("tp"),
        P(),
        P(),
        P("tp", None),
        P(),
        P(),
        P(None, EP),
        P(None, EP),
        P(EP, "tp"),
        P(EP, None),
        P(EP, None),
        P(EP, None, "tp"),
        P(EP, None, "tp"),
        P(EP, "tp", None),
    )

    return jax.shard_map(
        per_device, mesh=finer, in_specs=placed, out_specs=P(EP, "tp"), check_vma=False
    )
```

```python
import jax
import jax.numpy as jnp
from jax import lax
from jax.experimental import pallas as pl
from jax.experimental.pallas import tpu as pltpu
from jax.sharding import Mesh
from jax.sharding import PartitionSpec as P

EP = ("ep_0", "ep_1", "ep_2")
PAIR = "ep_2"
LANES = 128
NOTE_ROWS = 2

epsilon = 1e-06

VMEM = pl.BlockSpec(memory_space=pltpu.VMEM)
SMEM = pl.BlockSpec(memory_space=pltpu.SMEM)
ANY = pl.BlockSpec(memory_space=pl.ANY)


def swap(shard):
    return lax.ppermute(shard, PAIR, [(0, 1), (1, 0)])


def scaled(values, gain):
    mean = jnp.mean(values * values, axis=-1, keepdims=True)
    return values * lax.rsqrt(mean + epsilon) * gain


def silu(values):
    return values / (1.0 + jnp.exp(-values))


def in_vmem(values):
    return pltpu.with_memory_space_constraint(values, pltpu.VMEM)


def shifted(shard, step, members):
    pairs = []
    for core, sign in enumerate((1, -1)):
        for t in range(members):
            target = (t + sign * step) % members
            pairs.append((core * members + t, core * members + target))
    return lax.ppermute(shard, (PAIR, "tp"), pairs)


def wide_dot(left, right):
    return jnp.dot(left, right, preferred_element_type=jnp.float32)


def attend_kernel(*refs):
    inputs, outputs, scratch = refs[:20], refs[20:23], refs[23:]
    partial, packed, notes = outputs
    locals_, sems = scratch[:-1], scratch[-1]
    expert_gate, expert_up, expert_down, shared_down = inputs[16:]
    copies = []

    def start(source, target):
        copy = pltpu.make_async_copy(source, target, sems.at[len(copies)])
        copy.start()
        copies.append(copy)

    for source, target in zip(inputs[:16], locals_):
        start(source, target)
    tokens, norm_gain, query_weight, query_gain, key_weight, key_gain = locals_[:6]
    value_weight, forget_weight, forget_bias, keys, cum, lengths = locals_[6:12]
    values, out_weight, routes, route_weights = locals_[12:]
    first_packed = len(copies)
    row = 0

    def pack(source, row):
        start(source, packed.at[pl.ds(row, source.shape[0]), :])
        return row + source.shape[0]

    row = pack(expert_gate, row)
    row = pack(expert_up, row)
    for block in range(expert_down.shape[1] // LANES):
        row = pack(expert_down.at[:, pl.ds(block * LANES, LANES)], row)
    for block in range(shared_down.shape[1] // LANES):
        row = pack(shared_down.at[:, pl.ds(block * LANES, LANES)], row)

    seqs, cache_len, head = keys.shape
    groups = query_weight.shape[1] // head
    for copy in copies[:3]:
        copy.wait()
    normed = scaled(tokens[...].astype(jnp.float32), norm_gain[...].astype(jnp.float32))
    normed = normed.astype(jnp.bfloat16)
    for copy in copies[3:9]:
        copy.wait()
    gain = query_gain[...].astype(jnp.float32)
    wide = wide_dot(normed, query_weight[...])
    query = [scaled(wide[:, g * head : (g + 1) * head], gain) for g in range(groups)]
    query = jnp.concatenate(query, axis=0).astype(jnp.bfloat16)
    new_key = scaled(wide_dot(normed, key_weight[...]), key_gain[...].astype(jnp.float32))
    new_key = new_key.astype(jnp.bfloat16).astype(jnp.float32)
    new_value = wide_dot(normed, value_weight[...]).astype(jnp.bfloat16).astype(jnp.float32)
    products = normed.astype(jnp.float32) * forget_weight[...].astype(jnp.float32)
    forget = jnp.sum(products, axis=-1, keepdims=True) + forget_bias[0]
    new_log = jnp.minimum(forget, 0.0) - jnp.log1p(jnp.exp(-jnp.abs(forget)))

    rows = groups * seqs
    owner = lax.broadcasted_iota(jnp.int32, (rows, cache_len), 0) % seqs
    position = lax.broadcasted_iota(jnp.int32, (rows, cache_len), 1)
    scores = jnp.zeros((rows, cache_len), jnp.float32)
    decay = jnp.zeros((rows, cache_len), jnp.float32)
    length = jnp.zeros((rows, cache_len), jnp.int32)
    for copy in copies[9:12]:
        copy.wait()
    for b in range(seqs):
        mine = owner == b
        one = lax.dot_general(
            query, keys[b], (((1,), (1,)), ((), ())), preferred_element_type=jnp.float32
        )
        scores = jnp.where(mine, one, scores)
        decay = jnp.where(mine, cum[b], decay)
        length = jnp.where(mine, lengths[b], length)
    last = jnp.where(position == length - 1, decay, 0.0)
    last = jnp.sum(last, axis=-1, keepdims=True)
    bias = last - decay + jnp.concatenate([new_log] * groups, axis=0)
    score_scale = head ** (-0.5)
    past = jnp.where(position < length, scores * score_scale + bias, -jnp.inf)
    own = query.astype(jnp.float32) * jnp.concatenate([new_key] * groups, axis=0)
    own = jnp.sum(own, axis=-1, keepdims=True) * score_scale
    past_exp = jnp.exp(past)
    own_exp = jnp.exp(own)
    denominator = jnp.sum(past_exp, axis=-1, keepdims=True) + own_exp
    past_prob = (past_exp / denominator).astype(jnp.bfloat16)
    own_prob = (own_exp / denominator).astype(jnp.bfloat16).astype(jnp.float32)
    head_owner = owner[:, :head]
    mixed = jnp.zeros((rows, head), jnp.float32)
    copies[12].wait()
    for b in range(seqs):
        mixed = jnp.where(head_owner == b, wide_dot(past_prob, values[b]), mixed)
    mixed = mixed + own_prob * jnp.concatenate([new_value] * groups, axis=0)
    heads_out = [mixed[g * seqs : (g + 1) * seqs] for g in range(groups)]
    heads_out = jnp.concatenate(heads_out, axis=1).astype(jnp.bfloat16)
    copies[13].wait()
    product = wide_dot(heads_out, out_weight[...]).astype(jnp.bfloat16)
    for peer in range(partial.shape[0]):
        partial[peer] = product

    copies[14].wait()
    copies[15].wait()
    members = partial.shape[0]
    member = lax.axis_index("tp")
    norm_weights = route_weights[...]
    norm_weights = norm_weights / jnp.sum(norm_weights, axis=0, keepdims=True)
    high = norm_weights.astype(jnp.bfloat16).astype(jnp.float32)
    marks = (routes[...].astype(jnp.float32), high, norm_weights - high)
    column = lax.broadcasted_iota(jnp.int32, routes.shape, 1)
    lane = lax.broadcasted_iota(jnp.int32, (1, LANES), 1)
    lines = []
    for half in range(2):
        at = half * members + member
        line = jnp.zeros((1, LANES), jnp.float32)
        for i, mark in enumerate(marks):
            here = jnp.sum(jnp.where(column == at, mark, 0.0), axis=1, keepdims=True)
            for j in range(2):
                line = jnp.where(lane == 2 * i + j, here[j : j + 1], line)
        lines.append(line)
    notes[...] = jnp.concatenate(lines + [jnp.zeros((6, LANES), jnp.float32)], axis=0)
    for copy in copies[first_packed:]:
        copy.wait()


def rows_kernel(partial, tokens, ffn_gain, notes, residual, outgoing):
    member = lax.axis_index("tp")
    attended = jnp.sum(partial[...].astype(jnp.float32), axis=0)
    full = tokens[...].astype(jnp.float32) + attended
    seqs, width = full.shape
    members = partial.shape[0]
    slice_width = width // members
    for t in range(members):

        @pl.when(member == t)
        def _():
            residual[...] = full[:, t * slice_width : (t + 1) * slice_width]

    normed = scaled(full, ffn_gain[...].astype(jnp.float32))
    normed = normed.astype(jnp.bfloat16).astype(jnp.float32)
    rows_here = lax.broadcasted_iota(jnp.int32, (seqs, width), 0)
    pieces = []
    for half in range(2):
        at = half * members + member
        row = jnp.sum(jnp.where(rows_here == at, normed, 0.0), axis=0, keepdims=True)
        pieces += [row[:, k : k + LANES] for k in range(0, width, LANES)]
        pieces += [notes[half : half + 1, :], jnp.zeros((1, LANES), jnp.float32)]
    pattern = jnp.concatenate(pieces * 4, axis=0).astype(jnp.bfloat16)
    step = pattern.shape[0]
    for i in range(outgoing.shape[0] // step):
        outgoing[i * step : (i + 1) * step, :] = pattern


def share_kernel(rows, front, packed, *refs):
    sources, (out, wide, narrow, columns, staged, sems) = refs[:-6], refs[-6:]
    copies = []
    for i, source in enumerate(sources):
        copies.append(pltpu.make_async_copy(source, staged.at[i], sems.at[i]))
        copies[-1].start()
    packs = [packed] + [staged.at[i] for i in range(len(sources))]
    members = len(packs)
    member = lax.axis_index("tp")
    core = lax.axis_index(PAIR)
    me = lax.axis_index(EP).astype(jnp.float32)
    width = front.shape[1]
    count = narrow.shape[0]
    blocks = width // LANES
    stride = blocks + NOTE_ROWS
    lines = lax.axis_size("ep_1") * 2
    depth = count // lines
    wide[: rows.shape[0], :] = rows[...].astype(jnp.float32)
    marks = []
    for line in range(lines):
        for k in range(blocks + 1):
            piece = wide[pl.ds(line * stride + k, depth, stride=lines * stride), :]
            if k < blocks:
                at = (slice(line * depth, (line + 1) * depth), slice(k * LANES, (k + 1) * LANES))
                narrow[at] = piece.astype(jnp.bfloat16)
            else:
                marks.append(piece)
    marks = jnp.concatenate(marks, axis=0)
    weight = jnp.zeros((count, 1), jnp.float32)
    for j in range(2):
        norm_weight = marks[:, 2 + j : 3 + j] + marks[:, 4 + j : 5 + j]
        weight = weight + jnp.where(marks[:, j : j + 1] == me, norm_weight, 0.0)
    values = narrow[...]
    down_start = 2 * width
    shared_start = down_start + blocks * LANES
    per_member = blocks // members
    units = (packs[0].shape[0] - shared_start) // per_member

    pre = lax.dot_general(
        values, front[...], (((1,), (1,)), ((), ())), preferred_element_type=jnp.float32
    )
    mix_gate = 1.0 / (1.0 + jnp.exp(-pre[:, 2 * units : 2 * units + 1]))
    shared = (silu(pre[:, :units]) * pre[:, units : 2 * units]).astype(jnp.bfloat16)
    hidden = []
    for s in range(members):
        if s:
            copies[s - 1].wait()
        both = jnp.concatenate([packs[s][:width, :], packs[s][width : 2 * width, :]], axis=1)
        both = wide_dot(values, both)
        hidden.append((silu(both[:, :LANES]) * both[:, LANES:]).astype(jnp.bfloat16))
    halves = [jnp.concatenate(hidden[i : i + 2], axis=1) for i in range(0, members, 2)]
    ahead = jnp.where(core == 0, members - 1, 1)
    for s, origin in enumerate((0, ahead, members - ahead, 2)):
        dense = [
            packs[s][pl.ds(shared_start + k * units, units), :] for k in range(per_member)
        ]
        dense = wide_dot(shared, jnp.concatenate(dense, axis=1))
        columns[(member + origin) % members] = mix_gate * dense
    for n in range(members):
        firsts = [down_start + (n * per_member + k) * LANES for k in range(per_member)]
        total = columns[n]
        for i in range(len(halves)):
            down = [
                jnp.concatenate(
                    [packs[2 * i + s][first : first + LANES, :] for s in range(2)], axis=0
                )
                for first in firsts
            ]
            total = total + weight * wide_dot(halves[i], jnp.concatenate(down, axis=1))
        for k in range(per_member):
            for line in range(lines):
                first = line // 2 * depth * 2 * blocks + n * depth * 2 * per_member
                first = first + line % 2 * per_member + k
                piece = total[line * depth : (line + 1) * depth, k * LANES : (k + 1) * LANES]
                wide[pl.ds(first, depth, stride=2 * per_member), :] = piece
    out[...] = wide[: count * blocks, :].astype(out.dtype)


def add_kernel(own, pair, out):
    out[...] = (own[...] + pair[...].astype(jnp.float32)).astype(jnp.bfloat16)


def fold_kernel(parts, out, wide, small):
    sources = lax.axis_size("ep_1")
    members = lax.axis_size("tp")
    rows = parts.shape[0] // sources
    wide[...] = parts[...].astype(jnp.float32)
    total = wide[:rows, :]
    for i in range(1, sources):
        total = total + wide[i * rows : (i + 1) * rows, :]
    wide[:rows, :] = total
    halves = 2
    count = rows // members // halves
    for t in range(members):
        for j in range(halves):
            piece = wide[pl.ds(t * count * halves + j, count, stride=halves), :]
            small[pl.ds(t * halves + j, count, stride=members * halves), :] = piece
    out[...] = small[...].astype(jnp.bfloat16)


def finish_kernel(parts, residual, out, small):
    rows = small.shape[0]
    total = parts[:rows, :].astype(jnp.float32)
    for i in range(1, parts.shape[0] // rows):
        total = total + parts[i * rows : (i + 1) * rows, :].astype(jnp.float32)
    small[...] = total
    seqs = residual.shape[0]
    for j in range(rows // seqs):
        piece = small[pl.ds(j, seqs, stride=rows // seqs), :]
        columns = slice(j * LANES, (j + 1) * LANES)
        out[:, columns] = (residual[:, columns] + piece).astype(jnp.bfloat16)


def per_device(
    tokens,
    lengths,
    cache_keys,
    cache_values,
    cache_cum,
    norm_gain,
    query_weight,
    key_weight,
    value_weight,
    forget_weight,
    forget_bias,
    query_gain,
    key_gain,
    out_weight,
    ffn_gain,
    mix_weight,
    shared_gate,
    shared_up,
    shared_down,
    routes,
    route_weights,
    expert_gate,
    expert_up,
    expert_down,
):
    seqs, width = tokens.shape
    cache_len, head = cache_keys.shape[1], cache_keys.shape[3]
    peers = lax.axis_size(EP)
    members = lax.axis_size("tp")
    blocks = width // LANES
    units = shared_gate.shape[1]
    hidden = expert_gate.shape[2]
    pack_rows = 2 * width + hidden * blocks + units * shared_down.shape[1] // LANES
    copies = 2 + blocks + shared_down.shape[1] // LANES

    local = [
        tokens,
        norm_gain,
        query_weight,
        query_gain,
        key_weight,
        key_gain,
        value_weight,
        forget_weight.reshape(1, width),
        forget_bias,
        cache_keys.reshape(seqs, cache_len, head),
        cache_cum,
        lengths,
        cache_values.reshape(seqs, cache_len, head),
        out_weight,
        routes.T,
        route_weights.T,
    ]
    spaces = [pltpu.SMEM if each is forget_bias or each is lengths else pltpu.VMEM for each in local]
    partial, packed, notes = pl.pallas_call(
        attend_kernel,
        in_specs=[ANY] * (len(local) + 4),
        out_specs=[VMEM] * 3,
        out_shape=[
            pltpu.VMEM((members, seqs, width), jnp.bfloat16),
            pltpu.VMEM((pack_rows, LANES), jnp.bfloat16),
            pltpu.VMEM((8, LANES), jnp.float32),
        ],
        scratch_shapes=[space(each.shape, each.dtype) for space, each in zip(spaces, local)]
        + [pltpu.SemaphoreType.DMA((copies + len(local),))],
        name="attend",
    )(*local, expert_gate[0], expert_up[0], expert_down[0], shared_down)
    partial = lax.all_to_all(partial, "tp", 0, 0, tiled=True)
    ahead = shifted(packed, 1, members)
    behind = shifted(packed, -1, members)
    across = shifted(ahead, 1, members)
    packs = [packed, ahead, behind, across]

    front = [shared_gate.T, shared_up.T, mix_weight[None]]
    front = jnp.concatenate(front, axis=0)
    front = jnp.pad(front, ((0, LANES - front.shape[0]), (0, 0)))

    sub_rows = peers * (blocks + NOTE_ROWS)
    residual, outgoing = pl.pallas_call(
        rows_kernel,
        in_specs=[VMEM] * 4,
        out_specs=[VMEM, VMEM],
        out_shape=[
            pltpu.VMEM((seqs, width // members), jnp.float32),
            pltpu.VMEM((sub_rows, LANES), jnp.bfloat16),
        ],
        name="rows",
    )(*map(in_vmem, (partial, tokens, ffn_gain, notes)))
    own_rows = lax.all_to_all(outgoing.reshape(-1, 2, LANES), EP[:2], 0, 0, tiled=True)


    def share(rows, dtype):
        return pl.pallas_call(
            share_kernel,
            in_specs=[VMEM] * 3 + [ANY] * (members - 1),
            out_specs=VMEM,
            out_shape=pltpu.VMEM((peers * blocks, LANES), dtype),
            scratch_shapes=[
                pltpu.VMEM((sub_rows, LANES), jnp.float32),
                pltpu.VMEM((peers, width), jnp.bfloat16),
                pltpu.VMEM((members, peers, width // members), jnp.float32),
                pltpu.VMEM((members - 1, pack_rows, LANES), jnp.bfloat16),
                pltpu.SemaphoreType.DMA((members - 1,)),
            ],
            name="share",
        )(*map(in_vmem, (rows.reshape(sub_rows, LANES), front, packed)), *packs[1:])

    pair_rows = swap(own_rows)
    own_share = share(own_rows, jnp.float32)
    pair_share = share(pair_rows, jnp.bfloat16)
    pair_share = swap(pair_share)
    total = pl.pallas_call(
        add_kernel,
        in_specs=[VMEM] * 2,
        out_specs=VMEM,
        out_shape=pltpu.VMEM(own_share.shape, jnp.bfloat16),
        name="add",
    )(in_vmem(own_share), in_vmem(pair_share))
    parts = lax.all_to_all(total.reshape(-1, 2, LANES), ("ep_1", "tp"), 0, 0, tiled=True)
    parts = parts.reshape(-1, LANES)
    rows = parts.shape[0] // lax.axis_size("ep_1")
    parts = pl.pallas_call(
        fold_kernel,
        in_specs=[VMEM],
        out_specs=VMEM,
        out_shape=pltpu.VMEM((rows, LANES), jnp.bfloat16),
        scratch_shapes=[
            pltpu.VMEM(parts.shape, jnp.float32),
            pltpu.VMEM((rows, LANES), jnp.float32),
        ],
        name="fold",
    )(in_vmem(parts))
    parts = lax.all_to_all(parts.reshape(-1, 2, LANES), EP[0], 0, 0, tiled=True)
    return pl.pallas_call(
        finish_kernel,
        in_specs=[VMEM] * 2,
        out_specs=VMEM,
        out_shape=jax.ShapeDtypeStruct((seqs, width // members), jnp.bfloat16),
        scratch_shapes=[pltpu.VMEM((seqs * width // members // LANES, LANES), jnp.float32)],
        name="finish",
    )(in_vmem(parts.reshape(-1, LANES)), in_vmem(residual))


def solution(mesh):
    finer = Mesh(mesh.devices.reshape(16, 4, 2, mesh.shape["tp"]), ("ep_0", "ep_1", "ep_2", "tp"))
    placed = (
        P(EP, None),
        P(EP),
        P(EP, None, "tp", None),
        P(EP, None, "tp", None),
        P(EP, "tp", None),
        P(),
        P(None, "tp"),
        P(None, "tp"),
        P(None, "tp"),
        P(None, "tp"),
        P("tp"),
        P(),
        P(),
        P("tp", None),
        P(),
        P(),
        P(None, EP),
        P(None, EP),
        P(EP, "tp"),
        P(EP, None),
        P(EP, None),
        P(EP, None, "tp"),
        P(EP, None, "tp"),
        P(EP, "tp", None),
    )

    return jax.shard_map(
        per_device, mesh=finer, in_specs=placed, out_specs=P(EP, "tp"), check_vma=False
    )
```

```python
import jax
import jax.numpy as jnp
from jax import lax
from jax.experimental import pallas as pl
from jax.experimental.pallas import tpu as pltpu
from jax.sharding import Mesh
from jax.sharding import PartitionSpec as P

EP = ("ep_0", "ep_1", "ep_2")
PAIR = "ep_2"
LANES = 128

epsilon = 1e-06

VMEM = pl.BlockSpec(memory_space=pltpu.VMEM)
SMEM = pl.BlockSpec(memory_space=pltpu.SMEM)
ANY = pl.BlockSpec(memory_space=pl.ANY)


def swap(shard):
    return lax.ppermute(shard, PAIR, [(0, 1), (1, 0)])


def scaled(values, gain):
    mean = jnp.mean(values * values, axis=-1, keepdims=True)
    return values * lax.rsqrt(mean + epsilon) * gain


def silu(values):
    return values / (1.0 + jnp.exp(-values))


def in_vmem(values):
    return pltpu.with_memory_space_constraint(values, pltpu.VMEM)


def shifted(shard, step, members):
    pairs = []
    for core, sign in enumerate((1, -1)):
        for t in range(members):
            target = (t + sign * step) % members
            pairs.append((core * members + t, core * members + target))
    return lax.ppermute(shard, (PAIR, "tp"), pairs)


def wide_dot(left, right):
    return jnp.dot(left, right, preferred_element_type=jnp.float32)


def attend_kernel(*refs):
    inputs, outputs, scratch = refs[:20], refs[20:23], refs[23:]
    partial, packed, notes = outputs
    locals_, sems = scratch[:-1], scratch[-1]
    expert_gate, expert_up, expert_down, shared_down = inputs[16:]
    copies = []

    def start(source, target):
        copy = pltpu.make_async_copy(source, target, sems.at[len(copies)])
        copy.start()
        copies.append(copy)

    for source, target in zip(inputs[:16], locals_):
        start(source, target)
    tokens, norm_gain, query_weight, query_gain, key_weight, key_gain = locals_[:6]
    value_weight, forget_weight, forget_bias, keys, cum, lengths = locals_[6:12]
    values, out_weight, routes, route_weights = locals_[12:]
    first_packed = len(copies)
    row = 0

    def pack(source, row):
        start(source, packed.at[pl.ds(row, source.shape[0]), :])
        return row + source.shape[0]

    row = pack(expert_gate, row)
    row = pack(expert_up, row)
    for block in range(expert_down.shape[1] // LANES):
        row = pack(expert_down.at[:, pl.ds(block * LANES, LANES)], row)
    for block in range(shared_down.shape[1] // LANES):
        row = pack(shared_down.at[:, pl.ds(block * LANES, LANES)], row)

    seqs, cache_len, head = keys.shape
    groups = query_weight.shape[1] // head
    for copy in copies[:3]:
        copy.wait()
    normed = scaled(tokens[...].astype(jnp.float32), norm_gain[...].astype(jnp.float32))
    normed = normed.astype(jnp.bfloat16)
    for copy in copies[3:9]:
        copy.wait()
    gain = query_gain[...].astype(jnp.float32)
    wide = wide_dot(normed, query_weight[...])
    query = [scaled(wide[:, g * head : (g + 1) * head], gain) for g in range(groups)]
    query = jnp.concatenate(query, axis=0).astype(jnp.bfloat16)
    new_key = scaled(wide_dot(normed, key_weight[...]), key_gain[...].astype(jnp.float32))
    new_key = new_key.astype(jnp.bfloat16).astype(jnp.float32)
    new_value = wide_dot(normed, value_weight[...]).astype(jnp.bfloat16).astype(jnp.float32)
    products = normed.astype(jnp.float32) * forget_weight[...].astype(jnp.float32)
    forget = jnp.sum(products, axis=-1, keepdims=True) + forget_bias[0]
    new_log = jnp.minimum(forget, 0.0) - jnp.log1p(jnp.exp(-jnp.abs(forget)))

    rows = groups * seqs
    owner = lax.broadcasted_iota(jnp.int32, (rows, cache_len), 0) % seqs
    position = lax.broadcasted_iota(jnp.int32, (rows, cache_len), 1)
    scores = jnp.zeros((rows, cache_len), jnp.float32)
    decay = jnp.zeros((rows, cache_len), jnp.float32)
    length = jnp.zeros((rows, cache_len), jnp.int32)
    for copy in copies[9:12]:
        copy.wait()
    for b in range(seqs):
        mine = owner == b
        one = lax.dot_general(
            query, keys[b], (((1,), (1,)), ((), ())), preferred_element_type=jnp.float32
        )
        scores = jnp.where(mine, one, scores)
        decay = jnp.where(mine, cum[b], decay)
        length = jnp.where(mine, lengths[b], length)
    last = jnp.where(position == length - 1, decay, 0.0)
    last = jnp.sum(last, axis=-1, keepdims=True)
    bias = last - decay + jnp.concatenate([new_log] * groups, axis=0)
    score_scale = head ** (-0.5)
    past = jnp.where(position < length, scores * score_scale + bias, -jnp.inf)
    own = query.astype(jnp.float32) * jnp.concatenate([new_key] * groups, axis=0)
    own = jnp.sum(own, axis=-1, keepdims=True) * score_scale
    past_exp = jnp.exp(past)
    own_exp = jnp.exp(own)
    denominator = jnp.sum(past_exp, axis=-1, keepdims=True) + own_exp
    past_prob = (past_exp / denominator).astype(jnp.bfloat16)
    own_prob = (own_exp / denominator).astype(jnp.bfloat16).astype(jnp.float32)
    head_owner = owner[:, :head]
    mixed = jnp.zeros((rows, head), jnp.float32)
    copies[12].wait()
    for b in range(seqs):
        mixed = jnp.where(head_owner == b, wide_dot(past_prob, values[b]), mixed)
    mixed = mixed + own_prob * jnp.concatenate([new_value] * groups, axis=0)
    heads_out = [mixed[g * seqs : (g + 1) * seqs] for g in range(groups)]
    heads_out = jnp.concatenate(heads_out, axis=1).astype(jnp.bfloat16)
    copies[13].wait()
    product = wide_dot(heads_out, out_weight[...]).astype(jnp.bfloat16)
    for peer in range(partial.shape[0]):
        partial[peer] = product

    copies[14].wait()
    copies[15].wait()
    members = partial.shape[0]
    member = lax.axis_index("tp")
    norm_weights = route_weights[...]
    norm_weights = norm_weights / jnp.sum(norm_weights, axis=0, keepdims=True)
    high = norm_weights.astype(jnp.bfloat16).astype(jnp.float32)
    marks = (routes[...].astype(jnp.float32), high, norm_weights - high)
    column = lax.broadcasted_iota(jnp.int32, routes.shape, 1)
    lane = lax.broadcasted_iota(jnp.int32, (1, LANES), 1)
    lines = []
    for half in range(2):
        at = half * members + member
        line = jnp.zeros((1, LANES), jnp.float32)
        for i, mark in enumerate(marks):
            here = jnp.sum(jnp.where(column == at, mark, 0.0), axis=1, keepdims=True)
            for j in range(2):
                line = jnp.where(lane == 2 * i + j, here[j : j + 1], line)
        lines.append(line)
    notes[...] = jnp.concatenate(lines + [jnp.zeros((6, LANES), jnp.float32)], axis=0)
    for copy in copies[first_packed:]:
        copy.wait()


def rows_kernel(partial, tokens, ffn_gain, notes, residual, outgoing):
    member = lax.axis_index("tp")
    attended = jnp.sum(partial[...].astype(jnp.float32), axis=0)
    full = tokens[...].astype(jnp.float32) + attended
    seqs, width = full.shape
    members = partial.shape[0]
    slice_width = width // members
    for t in range(members):

        @pl.when(member == t)
        def _():
            residual[...] = full[:, t * slice_width : (t + 1) * slice_width]

    normed = scaled(full, ffn_gain[...].astype(jnp.float32))
    normed = normed.astype(jnp.bfloat16).astype(jnp.float32)
    rows_here = lax.broadcasted_iota(jnp.int32, (seqs, width), 0)
    pieces = []
    for half in range(2):
        at = half * members + member
        row = jnp.sum(jnp.where(rows_here == at, normed, 0.0), axis=0, keepdims=True)
        pieces += [row[:, k : k + LANES] for k in range(0, width, LANES)]
    pieces.append(notes[:2, :])
    pattern = jnp.concatenate(pieces * 8, axis=0).astype(jnp.bfloat16)
    step = pattern.shape[0]
    for i in range(outgoing.shape[0] // step):
        outgoing[i * step : (i + 1) * step, :] = pattern


def place_columns(target, values, n, depth, lines, blocks, per_member):
    for k in range(per_member):
        for line in range(lines):
            first = line // 2 * depth * 2 * blocks + n * depth * 2 * per_member
            first = first + line % 2 * per_member + k
            piece = values[line * depth : (line + 1) * depth, k * LANES : (k + 1) * LANES]
            target[pl.ds(first, depth, stride=2 * per_member), :] = piece


def hidden_of(values, pack, width):
    both = jnp.concatenate([pack[:width, :], pack[width : 2 * width, :]], axis=1)
    both = wide_dot(values, both)
    return (silu(both[:, :LANES]) * both[:, LANES:]).astype(jnp.bfloat16)


def down_of(packs, first, per_member):
    columns = []
    for k in range(per_member):
        rows = slice(first + k * LANES, first + (k + 1) * LANES)
        columns.append(jnp.concatenate([pack[rows, :] for pack in packs], axis=0))
    return jnp.concatenate(columns, axis=1)


def share_kernel(rows, front, pair_front, resident, *refs):
    sources, refs = refs[:-7], refs[-7:]
    out, narrow, aside, wide, columns, staged, sems = refs
    copies = []
    for i, source in enumerate(sources):
        copies.append(pltpu.make_async_copy(source, staged.at[i], sems.at[i]))
        copies[-1].start()
    members = lax.axis_size("tp")
    packs = [staged.at[i] for i in range(len(sources))]
    packs.insert(members, resident)
    member = lax.axis_index("tp")
    core = lax.axis_index(PAIR)
    experts = (lax.axis_index(EP), lax.axis_index(EP) + 1 - 2 * core)
    width = front.shape[1]
    count = narrow.shape[0]
    blocks = width // LANES
    stride = 2 * blocks + 2
    lines = lax.axis_size("ep_1") * 2
    depth = count // lines
    wide[: rows.shape[0], :] = rows[...].astype(jnp.float32)
    marks = []
    for line in range(lines):
        chip, half = line // 2, line % 2
        for k in range(blocks + 1):
            first = chip * stride + (half * blocks + k if k < blocks else 2 * blocks + half)
            piece = wide[pl.ds(first, depth, stride=lines // 2 * stride), :]
            if k < blocks:
                at = (slice(line * depth, (line + 1) * depth), slice(k * LANES, (k + 1) * LANES))
                narrow[at] = piece.astype(jnp.bfloat16)
            else:
                marks.append(piece)
    marks = jnp.concatenate(marks, axis=0)
    weights = []
    for expert in experts:
        weight = jnp.zeros((count, 1), jnp.float32)
        for j in range(2):
            norm_weight = marks[:, 2 + j : 3 + j] + marks[:, 4 + j : 5 + j]
            chosen = marks[:, j : j + 1] == expert.astype(jnp.float32)
            weight = weight + jnp.where(chosen, norm_weight, 0.0)
        weights.append(weight)
    values = narrow[...]
    down_start = 2 * width
    shared_start = down_start + blocks * LANES
    per_member = blocks // members
    units = (resident.shape[0] - shared_start) // per_member

    fronts = [
        lax.dot_general(
            values, each[...], (((1,), (1,)), ((), ())), preferred_element_type=jnp.float32
        )
        for each in (front, pair_front)
    ]
    mix_gate = 1.0 / (1.0 + jnp.exp(-fronts[0][:, 2 * units : 2 * units + 1]))
    shared = [silu(pre[:, :units]) * pre[:, units : 2 * units] for pre in fronts]
    shared = [each.astype(jnp.bfloat16) for each in shared]
    lane = lax.broadcasted_iota(jnp.int32, aside.shape, 1)
    scalars = jnp.where(lane == 0, weights[1], mix_gate)
    aside[...] = scalars
    aside[:, LANES - units :] = shared[1].astype(jnp.float32)

    hidden = []
    first_hidden = hidden_of(values, resident, width)
    for copy, pack in zip(copies, packs[:members] + packs[members + 1 :]):
        copy.wait()
        hidden.append(hidden_of(values, pack, width))
    hidden.insert(members, first_hidden)
    ahead = jnp.where(core == 0, members - 1, 1)
    origins = (0, ahead, members - ahead, 2)
    for s, pair in enumerate((0, 2, 1, None)):
        dense = wide_dot(shared[0], dense_of(packs[s], shared_start, units, per_member))
        if pair is not None:
            other = dense_of(packs[members + pair], shared_start, units, per_member)
            dense = dense + wide_dot(shared[1], other)
        columns[(member + origins[s]) % members] = mix_gate * dense
    for n in range(members):
        first = down_start + n * per_member * LANES
        total = columns[n]
        for side in range(2):
            routed = jnp.zeros((count, per_member * LANES), jnp.float32)
            for i in range(side * members, min((side + 1) * members, len(packs)), 2):
                group = packs[i : min(i + 2, len(packs))]
                left = jnp.concatenate(hidden[i : i + len(group)], axis=1)
                routed = routed + wide_dot(left, down_of(group, first, per_member))
            total = total + weights[side] * routed
        place_columns(out, total, n, depth, lines, blocks, per_member)


def dense_of(pack, shared_start, units, per_member):
    parts = [pack[pl.ds(shared_start + k * units, units), :] for k in range(per_member)]
    return jnp.concatenate(parts, axis=1)


def last_kernel(partial, narrow, aside, pack, out, wide, columns):
    members = lax.axis_size("tp")
    member = lax.axis_index("tp")
    count, width = narrow.shape
    blocks = width // LANES
    per_member = blocks // members
    lines = lax.axis_size("ep_1") * 2
    depth = count // lines
    down_start = 2 * width
    shared_start = down_start + blocks * LANES
    units = (pack.shape[0] - shared_start) // per_member
    weight = aside[:, 0:1]
    mix_gate = aside[:, 1:2]
    shared = aside[:, LANES - units :].astype(jnp.bfloat16)
    hidden = hidden_of(narrow[...], pack, width)
    dense = mix_gate * wide_dot(shared, dense_of(pack, shared_start, units, per_member))
    columns[...] = jnp.zeros(columns.shape, jnp.float32)
    columns[(member + 2) % members] = dense
    for n in range(members):
        first = down_start + n * per_member * LANES
        routed = wide_dot(hidden, down_of([pack], first, per_member))
        total = columns[n] + weight * routed
        place_columns(wide, total, n, depth, lines, blocks, per_member)
    out[...] = (partial[...] + wide[...]).astype(jnp.bfloat16)


def fold_kernel(parts, out, wide, small):
    sources = lax.axis_size("ep_1")
    members = lax.axis_size("tp")
    rows = parts.shape[0] // sources
    wide[...] = parts[...].astype(jnp.float32)
    total = wide[:rows, :]
    for i in range(1, sources):
        total = total + wide[i * rows : (i + 1) * rows, :]
    wide[:rows, :] = total
    halves = 2
    count = rows // members // halves
    for t in range(members):
        for j in range(halves):
            piece = wide[pl.ds(t * count * halves + j, count, stride=halves), :]
            small[pl.ds(t * halves + j, count, stride=members * halves), :] = piece
    out[...] = small[...].astype(jnp.bfloat16)


def finish_kernel(parts, residual, out, small):
    rows = small.shape[0]
    total = parts[:rows, :].astype(jnp.float32)
    for i in range(1, parts.shape[0] // rows):
        total = total + parts[i * rows : (i + 1) * rows, :].astype(jnp.float32)
    small[...] = total
    seqs = residual.shape[0]
    for j in range(rows // seqs):
        piece = small[pl.ds(j, seqs, stride=rows // seqs), :]
        columns = slice(j * LANES, (j + 1) * LANES)
        out[:, columns] = (residual[:, columns] + piece).astype(jnp.bfloat16)


def per_device(
    tokens,
    lengths,
    cache_keys,
    cache_values,
    cache_cum,
    norm_gain,
    query_weight,
    key_weight,
    value_weight,
    forget_weight,
    forget_bias,
    query_gain,
    key_gain,
    out_weight,
    ffn_gain,
    mix_weight,
    shared_gate,
    shared_up,
    shared_down,
    routes,
    route_weights,
    expert_gate,
    expert_up,
    expert_down,
):
    seqs, width = tokens.shape
    cache_len, head = cache_keys.shape[1], cache_keys.shape[3]
    peers = lax.axis_size(EP)
    members = lax.axis_size("tp")
    blocks = width // LANES
    units = shared_gate.shape[1]
    hidden = expert_gate.shape[2]
    pack_rows = 2 * width + hidden * blocks + units * shared_down.shape[1] // LANES
    copies = 2 + blocks + shared_down.shape[1] // LANES

    local = [
        tokens,
        norm_gain,
        query_weight,
        query_gain,
        key_weight,
        key_gain,
        value_weight,
        forget_weight.reshape(1, width),
        forget_bias,
        cache_keys.reshape(seqs, cache_len, head),
        cache_cum,
        lengths,
        cache_values.reshape(seqs, cache_len, head),
        out_weight,
        routes.T,
        route_weights.T,
    ]
    spaces = [pltpu.SMEM if each is forget_bias or each is lengths else pltpu.VMEM for each in local]
    partial, packed, notes = pl.pallas_call(
        attend_kernel,
        in_specs=[ANY] * (len(local) + 4),
        out_specs=[VMEM] * 3,
        out_shape=[
            pltpu.VMEM((members, seqs, width), jnp.bfloat16),
            pltpu.VMEM((pack_rows, LANES), jnp.bfloat16),
            pltpu.VMEM((8, LANES), jnp.float32),
        ],
        scratch_shapes=[space(each.shape, each.dtype) for space, each in zip(spaces, local)]
        + [pltpu.SemaphoreType.DMA((copies + len(local),))],
        name="attend",
    )(*local, expert_gate[0], expert_up[0], expert_down[0], shared_down)
    partial = lax.all_to_all(partial, "tp", 0, 0, tiled=True)
    ahead = shifted(packed, 1, members)
    behind = shifted(packed, -1, members)
    across = shifted(ahead, 1, members)
    packs = [packed, ahead, behind, across]

    front = [shared_gate.T, shared_up.T, mix_weight[None]]
    front = jnp.concatenate(front, axis=0)
    front = jnp.pad(front, ((0, LANES - front.shape[0]), (0, 0)))

    sub_rows = peers * (blocks + 1)
    residual, outgoing = pl.pallas_call(
        rows_kernel,
        in_specs=[VMEM] * 4,
        out_specs=[VMEM, VMEM],
        out_shape=[
            pltpu.VMEM((seqs, width // members), jnp.float32),
            pltpu.VMEM((sub_rows, LANES), jnp.bfloat16),
        ],
        name="rows",
    )(*map(in_vmem, (partial, tokens, ffn_gain, notes)))
    own_rows = lax.all_to_all(outgoing.reshape(-1, 2, LANES), EP[:2], 0, 0, tiled=True)


    pair_front = swap(front)
    pair_packs = []
    for pack in packs:
        pair_packs.append(swap(pack))
    streamed = packs + pair_packs[1:-1]
    local_columns = pltpu.VMEM((members, peers, width // members), jnp.float32)
    partial_share, narrow, aside = pl.pallas_call(
        share_kernel,
        in_specs=[VMEM] * 4 + [ANY] * len(streamed),
        out_specs=[VMEM] * 3,
        out_shape=[
            pltpu.VMEM((peers * blocks, LANES), jnp.float32),
            pltpu.VMEM((peers, width), jnp.bfloat16),
            pltpu.VMEM((peers, LANES), jnp.float32),
        ],
        scratch_shapes=[
            pltpu.VMEM((sub_rows, LANES), jnp.float32),
            local_columns,
            pltpu.VMEM((len(streamed), pack_rows, LANES), jnp.bfloat16),
            pltpu.SemaphoreType.DMA((len(streamed),)),
        ],
        name="share",
    )(
        *map(in_vmem, (own_rows.reshape(sub_rows, LANES), front, pair_front, pair_packs[0])),
        *streamed,
    )
    total = pl.pallas_call(
        last_kernel,
        in_specs=[VMEM] * 4,
        out_specs=VMEM,
        out_shape=pltpu.VMEM((peers * blocks, LANES), jnp.bfloat16),
        scratch_shapes=[pltpu.VMEM((peers * blocks, LANES), jnp.float32), local_columns],
        name="last",
    )(*map(in_vmem, (partial_share, narrow, aside)), pair_packs[-1])
    parts = lax.all_to_all(total.reshape(-1, 2, LANES), ("ep_1", "tp"), 0, 0, tiled=True)
    parts = parts.reshape(-1, LANES)
    rows = parts.shape[0] // lax.axis_size("ep_1")
    parts = pl.pallas_call(
        fold_kernel,
        in_specs=[VMEM],
        out_specs=VMEM,
        out_shape=pltpu.VMEM((rows, LANES), jnp.bfloat16),
        scratch_shapes=[
            pltpu.VMEM(parts.shape, jnp.float32),
            pltpu.VMEM((rows, LANES), jnp.float32),
        ],
        name="fold",
    )(in_vmem(parts))
    parts = lax.all_to_all(parts.reshape(-1, 2, LANES), EP[0], 0, 0, tiled=True)
    return pl.pallas_call(
        finish_kernel,
        in_specs=[VMEM] * 2,
        out_specs=VMEM,
        out_shape=jax.ShapeDtypeStruct((seqs, width // members), jnp.bfloat16),
        scratch_shapes=[pltpu.VMEM((seqs * width // members // LANES, LANES), jnp.float32)],
        name="finish",
    )(in_vmem(parts.reshape(-1, LANES)), in_vmem(residual))


def solution(mesh):
    finer = Mesh(mesh.devices.reshape(16, 4, 2, mesh.shape["tp"]), ("ep_0", "ep_1", "ep_2", "tp"))
    placed = (
        P(EP, None),
        P(EP),
        P(EP, None, "tp", None),
        P(EP, None, "tp", None),
        P(EP, "tp", None),
        P(),
        P(None, "tp"),
        P(None, "tp"),
        P(None, "tp"),
        P(None, "tp"),
        P("tp"),
        P(),
        P(),
        P("tp", None),
        P(),
        P(),
        P(None, EP),
        P(None, EP),
        P(EP, "tp"),
        P(EP, None),
        P(EP, None),
        P(EP, None, "tp"),
        P(EP, None, "tp"),
        P(EP, "tp", None),
    )

    return jax.shard_map(
        per_device, mesh=finer, in_specs=placed, out_specs=P(EP, "tp"), check_vma=False
    )
```

```python
import jax
import jax.numpy as jnp
from jax import lax
from jax.experimental import pallas as pl
from jax.experimental.pallas import tpu as pltpu
from jax.sharding import Mesh
from jax.sharding import PartitionSpec as P

EP = ("ep_0", "ep_1", "ep_2")
PAIR = "ep_2"
LANES = 128

epsilon = 1e-06

VMEM = pl.BlockSpec(memory_space=pltpu.VMEM)
SMEM = pl.BlockSpec(memory_space=pltpu.SMEM)
ANY = pl.BlockSpec(memory_space=pl.ANY)


def swap(shard):
    return lax.ppermute(shard, PAIR, [(0, 1), (1, 0)])


def scaled(values, gain):
    mean = jnp.mean(values * values, axis=-1, keepdims=True)
    return values * lax.rsqrt(mean + epsilon) * gain


def silu(values):
    return values / (1.0 + jnp.exp(-values))


def in_vmem(values):
    return pltpu.with_memory_space_constraint(values, pltpu.VMEM)


def shifted(shard, step, members):
    pairs = []
    for core, sign in enumerate((1, -1)):
        for t in range(members):
            target = (t + sign * step) % members
            pairs.append((core * members + t, core * members + target))
    return lax.ppermute(shard, (PAIR, "tp"), pairs)


def wide_dot(left, right):
    return jnp.dot(left, right, preferred_element_type=jnp.float32)


def attend_kernel(*refs):
    inputs, outputs, scratch = refs[:20], refs[20:23], refs[23:]
    partial, packed, notes = outputs
    locals_, sems = scratch[:-1], scratch[-1]
    expert_gate, expert_up, expert_down, shared_down = inputs[16:]
    copies = []

    def start(source, target):
        copy = pltpu.make_async_copy(source, target, sems.at[len(copies)])
        copy.start()
        copies.append(copy)

    for source, target in zip(inputs[:16], locals_):
        start(source, target)
    tokens, norm_gain, query_weight, query_gain, key_weight, key_gain = locals_[:6]
    value_weight, forget_weight, forget_bias, keys, cum, lengths = locals_[6:12]
    values, out_weight, routes, route_weights = locals_[12:]
    first_packed = len(copies)
    row = 0

    def pack(source, row):
        start(source, packed.at[pl.ds(row, source.shape[0]), :])
        return row + source.shape[0]

    row = pack(expert_gate, row)
    row = pack(expert_up, row)
    for block in range(expert_down.shape[1] // LANES):
        row = pack(expert_down.at[:, pl.ds(block * LANES, LANES)], row)
    for block in range(shared_down.shape[1] // LANES):
        row = pack(shared_down.at[:, pl.ds(block * LANES, LANES)], row)

    seqs, cache_len, head = keys.shape
    groups = query_weight.shape[1] // head
    for copy in copies[:3]:
        copy.wait()
    normed = scaled(tokens[...].astype(jnp.float32), norm_gain[...].astype(jnp.float32))
    normed = normed.astype(jnp.bfloat16)
    for copy in copies[3:9]:
        copy.wait()
    gain = query_gain[...].astype(jnp.float32)
    wide = wide_dot(normed, query_weight[...])
    query = [scaled(wide[:, g * head : (g + 1) * head], gain) for g in range(groups)]
    query = jnp.concatenate(query, axis=0).astype(jnp.bfloat16)
    new_key = scaled(wide_dot(normed, key_weight[...]), key_gain[...].astype(jnp.float32))
    new_key = new_key.astype(jnp.bfloat16).astype(jnp.float32)
    new_value = wide_dot(normed, value_weight[...]).astype(jnp.bfloat16).astype(jnp.float32)
    products = normed.astype(jnp.float32) * forget_weight[...].astype(jnp.float32)
    forget = jnp.sum(products, axis=-1, keepdims=True) + forget_bias[0]
    new_log = jnp.minimum(forget, 0.0) - jnp.log1p(jnp.exp(-jnp.abs(forget)))

    rows = groups * seqs
    owner = lax.broadcasted_iota(jnp.int32, (rows, cache_len), 0) % seqs
    position = lax.broadcasted_iota(jnp.int32, (rows, cache_len), 1)
    scores = jnp.zeros((rows, cache_len), jnp.float32)
    decay = jnp.zeros((rows, cache_len), jnp.float32)
    length = jnp.zeros((rows, cache_len), jnp.int32)
    for copy in copies[9:12]:
        copy.wait()
    for b in range(seqs):
        mine = owner == b
        one = lax.dot_general(
            query, keys[b], (((1,), (1,)), ((), ())), preferred_element_type=jnp.float32
        )
        scores = jnp.where(mine, one, scores)
        decay = jnp.where(mine, cum[b], decay)
        length = jnp.where(mine, lengths[b], length)
    last = jnp.where(position == length - 1, decay, 0.0)
    last = jnp.sum(last, axis=-1, keepdims=True)
    bias = last - decay + jnp.concatenate([new_log] * groups, axis=0)
    score_scale = head ** (-0.5)
    past = jnp.where(position < length, scores * score_scale + bias, -jnp.inf)
    own = query.astype(jnp.float32) * jnp.concatenate([new_key] * groups, axis=0)
    own = jnp.sum(own, axis=-1, keepdims=True) * score_scale
    past_exp = jnp.exp(past)
    own_exp = jnp.exp(own)
    denominator = jnp.sum(past_exp, axis=-1, keepdims=True) + own_exp
    past_prob = (past_exp / denominator).astype(jnp.bfloat16)
    own_prob = (own_exp / denominator).astype(jnp.bfloat16).astype(jnp.float32)
    head_owner = owner[:, :head]
    mixed = jnp.zeros((rows, head), jnp.float32)
    copies[12].wait()
    for b in range(seqs):
        mixed = jnp.where(head_owner == b, wide_dot(past_prob, values[b]), mixed)
    mixed = mixed + own_prob * jnp.concatenate([new_value] * groups, axis=0)
    heads_out = [mixed[g * seqs : (g + 1) * seqs] for g in range(groups)]
    heads_out = jnp.concatenate(heads_out, axis=1).astype(jnp.bfloat16)
    copies[13].wait()
    product = wide_dot(heads_out, out_weight[...]).astype(jnp.bfloat16)
    for peer in range(partial.shape[0]):
        partial[peer] = product

    copies[14].wait()
    copies[15].wait()
    members = partial.shape[0]
    member = lax.axis_index("tp")
    norm_weights = route_weights[...]
    norm_weights = norm_weights / jnp.sum(norm_weights, axis=0, keepdims=True)
    high = norm_weights.astype(jnp.bfloat16).astype(jnp.float32)
    marks = (routes[...].astype(jnp.float32), high, norm_weights - high)
    column = lax.broadcasted_iota(jnp.int32, routes.shape, 1)
    lane = lax.broadcasted_iota(jnp.int32, (1, LANES), 1)
    lines = []
    for half in range(2):
        at = half * members + member
        line = jnp.zeros((1, LANES), jnp.float32)
        for i, mark in enumerate(marks):
            here = jnp.sum(jnp.where(column == at, mark, 0.0), axis=1, keepdims=True)
            for j in range(2):
                line = jnp.where(lane == 2 * i + j, here[j : j + 1], line)
        lines.append(line)
    notes[...] = jnp.concatenate(lines + [jnp.zeros((6, LANES), jnp.float32)], axis=0)
    for copy in copies[first_packed:]:
        copy.wait()


def rows_kernel(partial, tokens, ffn_gain, notes, residual, outgoing):
    member = lax.axis_index("tp")
    attended = jnp.sum(partial[...].astype(jnp.float32), axis=0)
    full = tokens[...].astype(jnp.float32) + attended
    seqs, width = full.shape
    members = partial.shape[0]
    slice_width = width // members
    for t in range(members):

        @pl.when(member == t)
        def _():
            residual[...] = full[:, t * slice_width : (t + 1) * slice_width]

    normed = scaled(full, ffn_gain[...].astype(jnp.float32))
    normed = normed.astype(jnp.bfloat16).astype(jnp.float32)
    rows_here = lax.broadcasted_iota(jnp.int32, (seqs, width), 0)
    pieces = []
    for half in range(2):
        at = half * members + member
        row = jnp.sum(jnp.where(rows_here == at, normed, 0.0), axis=0, keepdims=True)
        pieces += [row[:, k : k + LANES] for k in range(0, width, LANES)]
    pieces.append(notes[:2, :])
    pattern = jnp.concatenate(pieces * 8, axis=0).astype(jnp.bfloat16)
    step = pattern.shape[0]
    for i in range(outgoing.shape[0] // step):
        outgoing[i * step : (i + 1) * step, :] = pattern


def place_columns(target, values, n, depth, lines, blocks, per_member):
    for k in range(per_member):
        for line in range(lines):
            first = line // 2 * depth * 2 * blocks + n * depth * 2 * per_member
            first = first + line % 2 * per_member + k
            piece = values[line * depth : (line + 1) * depth, k * LANES : (k + 1) * LANES]
            target[pl.ds(first, depth, stride=2 * per_member), :] = piece


def hidden_of(values, pack, width):
    both = jnp.concatenate([pack[:width, :], pack[width : 2 * width, :]], axis=1)
    both = wide_dot(values, both)
    return (silu(both[:, :LANES]) * both[:, LANES:]).astype(jnp.bfloat16)


def down_of(packs, first, per_member):
    columns = []
    for k in range(per_member):
        rows = slice(first + k * LANES, first + (k + 1) * LANES)
        columns.append(jnp.concatenate([pack[rows, :] for pack in packs], axis=0))
    return jnp.concatenate(columns, axis=1)


def share_kernel(rows, resident, *refs):
    sources, refs = refs[:-10], refs[-10:]
    out, narrow, aside, wide, columns, staged, fronts_in, marks_in, sems, front_sems = refs
    copies = []
    for i, source in enumerate(sources[2:]):
        copies.append(pltpu.make_async_copy(source, staged.at[i], sems.at[i]))
    front_copies = []
    for i, source in enumerate(sources[:2]):
        front_copies.append(pltpu.make_async_copy(source, fronts_in.at[i], front_sems.at[i]))
    for copy in copies[:1] + front_copies + copies[1:]:
        copy.start()
    members = lax.axis_size("tp")
    packs = [resident] + [staged.at[i] for i in range(len(copies))]
    member = lax.axis_index("tp")
    core = lax.axis_index(PAIR)
    experts = (lax.axis_index(EP), lax.axis_index(EP) + 1 - 2 * core)
    width = fronts_in.shape[2]
    count = narrow.shape[0]
    blocks = width // LANES
    stride = 2 * blocks + 2
    lines = lax.axis_size("ep_1") * 2
    depth = count // lines
    share_rows = rows.shape[0] // lines

    @pl.loop(0, lines)
    def _(line):
        at = pl.ds(pl.multiple_of(line * share_rows, share_rows), share_rows)
        wide[at, :] = rows[at, :].astype(jnp.float32)

    @pl.loop(0, lines)
    def _(line):
        chip, half = line // 2, line % 2
        at = pl.ds(pl.multiple_of(line * depth, depth), depth)
        for k in range(blocks):
            first = chip * stride + half * blocks + k
            piece = wide[pl.ds(first, depth, stride=lines // 2 * stride), :]
            narrow[at, k * LANES : (k + 1) * LANES] = piece.astype(jnp.bfloat16)
        first = chip * stride + 2 * blocks + half
        marks_in[at, :] = wide[pl.ds(first, depth, stride=lines // 2 * stride), :]

    marks = marks_in[...]
    weights = []
    for expert in experts:
        weight = jnp.zeros((count, 1), jnp.float32)
        for j in range(2):
            norm_weight = marks[:, 2 + j : 3 + j] + marks[:, 4 + j : 5 + j]
            chosen = marks[:, j : j + 1] == expert.astype(jnp.float32)
            weight = weight + jnp.where(chosen, norm_weight, 0.0)
        weights.append(weight)
    values = narrow[...]
    down_start = 2 * width
    shared_start = down_start + blocks * LANES
    per_member = blocks // members
    units = (resident.shape[0] - shared_start) // per_member

    hidden = [hidden_of(values, resident, width)]
    for copy in front_copies:
        copy.wait()
    fronts = [
        lax.dot_general(
            values, each[...], (((1,), (1,)), ((), ())), preferred_element_type=jnp.float32
        )
        for each in (fronts_in.at[0], fronts_in.at[1])
    ]
    mix_gate = 1.0 / (1.0 + jnp.exp(-fronts[0][:, 2 * units : 2 * units + 1]))
    shared = [silu(pre[:, :units]) * pre[:, units : 2 * units] for pre in fronts]
    shared = [each.astype(jnp.bfloat16) for each in shared]
    lane = lax.broadcasted_iota(jnp.int32, aside.shape, 1)
    scalars = jnp.where(lane == 0, weights[1], mix_gate)
    aside[...] = scalars
    aside[:, LANES - units :] = shared[1].astype(jnp.float32)

    for copy, pack in zip(copies, packs[1:]):
        copy.wait()
        hidden.append(hidden_of(values, pack, width))
    ahead = jnp.where(core == 0, members - 1, 1)
    origins = (0, ahead, members - ahead, 2)
    for s, pair in enumerate((0, 2, 1, None)):
        dense = wide_dot(shared[0], dense_of(packs[s], shared_start, units, per_member))
        if pair is not None:
            other = dense_of(packs[members + pair], shared_start, units, per_member)
            dense = dense + wide_dot(shared[1], other)
        columns[(member + origins[s]) % members] = mix_gate * dense
    for n in range(members):
        first = down_start + n * per_member * LANES
        total = columns[n]
        for side in range(2):
            routed = jnp.zeros((count, per_member * LANES), jnp.float32)
            for i in range(side * members, min((side + 1) * members, len(packs)), 2):
                group = packs[i : min(i + 2, len(packs))]
                left = jnp.concatenate(hidden[i : i + len(group)], axis=1)
                routed = routed + wide_dot(left, down_of(group, first, per_member))
            total = total + weights[side] * routed
        place_columns(out, total, n, depth, lines, blocks, per_member)


def dense_of(pack, shared_start, units, per_member):
    parts = [pack[pl.ds(shared_start + k * units, units), :] for k in range(per_member)]
    return jnp.concatenate(parts, axis=1)


def last_kernel(partial, narrow, aside, source, out, wide, columns, pack, sems):
    split = 2 * narrow.shape[1]
    copies = []
    for i, rows in enumerate((pl.ds(0, split), pl.ds(split, source.shape[0] - split))):
        copies.append(pltpu.make_async_copy(source.at[rows, :], pack.at[rows, :], sems.at[i]))
        copies[-1].start()
    members = lax.axis_size("tp")
    member = lax.axis_index("tp")
    count, width = narrow.shape
    blocks = width // LANES
    per_member = blocks // members
    lines = lax.axis_size("ep_1") * 2
    depth = count // lines
    down_start = 2 * width
    shared_start = down_start + blocks * LANES
    units = (pack.shape[0] - shared_start) // per_member
    weight = aside[:, 0:1]
    mix_gate = aside[:, 1:2]
    shared = aside[:, LANES - units :].astype(jnp.bfloat16)
    copies[0].wait()
    hidden = hidden_of(narrow[...], pack, width)
    copies[1].wait()
    dense = mix_gate * wide_dot(shared, dense_of(pack, shared_start, units, per_member))
    columns[...] = jnp.zeros(columns.shape, jnp.float32)
    columns[(member + 2) % members] = dense
    for n in range(members):
        first = down_start + n * per_member * LANES
        routed = wide_dot(hidden, down_of([pack], first, per_member))
        total = columns[n] + weight * routed
        place_columns(wide, total, n, depth, lines, blocks, per_member)
    out[...] = (partial[...] + wide[...]).astype(jnp.bfloat16)


def fold_kernel(parts, out, wide, small):
    sources = lax.axis_size("ep_1")
    members = lax.axis_size("tp")
    rows = parts.shape[0] // sources
    wide[...] = parts[...].astype(jnp.float32)
    total = wide[:rows, :]
    for i in range(1, sources):
        total = total + wide[i * rows : (i + 1) * rows, :]
    wide[:rows, :] = total
    halves = 2
    count = rows // members // halves
    for t in range(members):
        for j in range(halves):
            piece = wide[pl.ds(t * count * halves + j, count, stride=halves), :]
            small[pl.ds(t * halves + j, count, stride=members * halves), :] = piece
    out[...] = small[...].astype(jnp.bfloat16)


def finish_kernel(parts, residual, out, small):
    rows = small.shape[0]
    total = parts[:rows, :].astype(jnp.float32)
    for i in range(1, parts.shape[0] // rows):
        total = total + parts[i * rows : (i + 1) * rows, :].astype(jnp.float32)
    small[...] = total
    seqs = residual.shape[0]
    for j in range(rows // seqs):
        piece = small[pl.ds(j, seqs, stride=rows // seqs), :]
        columns = slice(j * LANES, (j + 1) * LANES)
        out[:, columns] = (residual[:, columns] + piece).astype(jnp.bfloat16)


def per_device(
    tokens,
    lengths,
    cache_keys,
    cache_values,
    cache_cum,
    norm_gain,
    query_weight,
    key_weight,
    value_weight,
    forget_weight,
    forget_bias,
    query_gain,
    key_gain,
    out_weight,
    ffn_gain,
    mix_weight,
    shared_gate,
    shared_up,
    shared_down,
    routes,
    route_weights,
    expert_gate,
    expert_up,
    expert_down,
):
    seqs, width = tokens.shape
    cache_len, head = cache_keys.shape[1], cache_keys.shape[3]
    peers = lax.axis_size(EP)
    members = lax.axis_size("tp")
    blocks = width // LANES
    units = shared_gate.shape[1]
    hidden = expert_gate.shape[2]
    pack_rows = 2 * width + hidden * blocks + units * shared_down.shape[1] // LANES
    copies = 2 + blocks + shared_down.shape[1] // LANES

    local = [
        tokens,
        norm_gain,
        query_weight,
        query_gain,
        key_weight,
        key_gain,
        value_weight,
        forget_weight.reshape(1, width),
        forget_bias,
        cache_keys.reshape(seqs, cache_len, head),
        cache_cum,
        lengths,
        cache_values.reshape(seqs, cache_len, head),
        out_weight,
        routes.T,
        route_weights.T,
    ]
    spaces = [pltpu.SMEM if each is forget_bias or each is lengths else pltpu.VMEM for each in local]
    partial, packed, notes = pl.pallas_call(
        attend_kernel,
        in_specs=[ANY] * (len(local) + 4),
        out_specs=[VMEM] * 3,
        out_shape=[
            pltpu.VMEM((members, seqs, width), jnp.bfloat16),
            pltpu.VMEM((pack_rows, LANES), jnp.bfloat16),
            pltpu.VMEM((8, LANES), jnp.float32),
        ],
        scratch_shapes=[space(each.shape, each.dtype) for space, each in zip(spaces, local)]
        + [pltpu.SemaphoreType.DMA((copies + len(local),))],
        name="attend",
    )(*local, expert_gate[0], expert_up[0], expert_down[0], shared_down)
    partial = lax.all_to_all(partial, "tp", 0, 0, tiled=True)
    ahead = shifted(packed, 1, members)
    behind = shifted(packed, -1, members)
    across = shifted(ahead, 1, members)
    packs = [packed, ahead, behind, across]

    front = [shared_gate.T, shared_up.T, mix_weight[None]]
    front = jnp.concatenate(front, axis=0)
    front = jnp.pad(front, ((0, LANES - front.shape[0]), (0, 0)))

    sub_rows = peers * (blocks + 1)
    residual, outgoing = pl.pallas_call(
        rows_kernel,
        in_specs=[VMEM] * 4,
        out_specs=[VMEM, VMEM],
        out_shape=[
            pltpu.VMEM((seqs, width // members), jnp.float32),
            pltpu.VMEM((sub_rows, LANES), jnp.bfloat16),
        ],
        name="rows",
    )(*map(in_vmem, (partial, tokens, ffn_gain, notes)))
    own_rows = lax.all_to_all(outgoing.reshape(-1, 2, LANES), EP[:2], 0, 0, tiled=True)


    pair_front = swap(front)
    pair_packs = []
    for pack in packs:
        pair_packs.append(swap(pack))
    streamed = packs[1:] + pair_packs[:-1]
    local_columns = pltpu.VMEM((members, peers, width // members), jnp.float32)
    partial_share, narrow, aside = pl.pallas_call(
        share_kernel,
        in_specs=[VMEM] * 2 + [ANY] * (2 + len(streamed)),
        out_specs=[VMEM] * 3,
        out_shape=[
            pltpu.VMEM((peers * blocks, LANES), jnp.float32),
            pltpu.VMEM((peers, width), jnp.bfloat16),
            pltpu.VMEM((peers, LANES), jnp.float32),
        ],
        scratch_shapes=[
            pltpu.VMEM((sub_rows, LANES), jnp.float32),
            local_columns,
            pltpu.VMEM((len(streamed), pack_rows, LANES), jnp.bfloat16),
            pltpu.VMEM((2, LANES, width), jnp.bfloat16),
            pltpu.VMEM((peers, LANES), jnp.float32),
            pltpu.SemaphoreType.DMA((len(streamed),)),
            pltpu.SemaphoreType.DMA((2,)),
        ],
        name="share",
    )(
        *map(in_vmem, (own_rows.reshape(sub_rows, LANES), packed)),
        front,
        pair_front,
        *streamed,
    )
    total = pl.pallas_call(
        last_kernel,
        in_specs=[VMEM] * 3 + [ANY],
        out_specs=VMEM,
        out_shape=pltpu.VMEM((peers * blocks, LANES), jnp.bfloat16),
        scratch_shapes=[
            pltpu.VMEM((peers * blocks, LANES), jnp.float32),
            local_columns,
            pltpu.VMEM((pack_rows, LANES), jnp.bfloat16),
            pltpu.SemaphoreType.DMA((2,)),
        ],
        name="last",
    )(*map(in_vmem, (partial_share, narrow, aside)), pair_packs[-1])
    parts = lax.all_to_all(total.reshape(-1, 2, LANES), ("ep_1", "tp"), 0, 0, tiled=True)
    parts = parts.reshape(-1, LANES)
    rows = parts.shape[0] // lax.axis_size("ep_1")
    parts = pl.pallas_call(
        fold_kernel,
        in_specs=[VMEM],
        out_specs=VMEM,
        out_shape=pltpu.VMEM((rows, LANES), jnp.bfloat16),
        scratch_shapes=[
            pltpu.VMEM(parts.shape, jnp.float32),
            pltpu.VMEM((rows, LANES), jnp.float32),
        ],
        name="fold",
    )(in_vmem(parts))
    parts = lax.all_to_all(parts.reshape(-1, 2, LANES), EP[0], 0, 0, tiled=True)
    return pl.pallas_call(
        finish_kernel,
        in_specs=[VMEM] * 2,
        out_specs=VMEM,
        out_shape=jax.ShapeDtypeStruct((seqs, width // members), jnp.bfloat16),
        scratch_shapes=[pltpu.VMEM((seqs * width // members // LANES, LANES), jnp.float32)],
        name="finish",
    )(in_vmem(parts.reshape(-1, LANES)), in_vmem(residual))


def solution(mesh):
    finer = Mesh(mesh.devices.reshape(16, 4, 2, mesh.shape["tp"]), ("ep_0", "ep_1", "ep_2", "tp"))
    placed = (
        P(EP, None),
        P(EP),
        P(EP, None, "tp", None),
        P(EP, None, "tp", None),
        P(EP, "tp", None),
        P(),
        P(None, "tp"),
        P(None, "tp"),
        P(None, "tp"),
        P(None, "tp"),
        P("tp"),
        P(),
        P(),
        P("tp", None),
        P(),
        P(),
        P(None, EP),
        P(None, EP),
        P(EP, "tp"),
        P(EP, None),
        P(EP, None),
        P(EP, None, "tp"),
        P(EP, None, "tp"),
        P(EP, "tp", None),
    )

    return jax.shard_map(
        per_device, mesh=finer, in_specs=placed, out_specs=P(EP, "tp"), check_vma=False
    )
```

```python
import jax
import jax.numpy as jnp
from jax import lax
from jax.experimental import pallas as pl
from jax.experimental.pallas import tpu as pltpu
from jax.sharding import Mesh
from jax.sharding import PartitionSpec as P

EP = ("ep_0", "ep_1", "ep_2")
PAIR = "ep_2"
LANES = 128

epsilon = 1e-06

VMEM = pl.BlockSpec(memory_space=pltpu.VMEM)
SMEM = pl.BlockSpec(memory_space=pltpu.SMEM)
ANY = pl.BlockSpec(memory_space=pl.ANY)


def swap(shard):
    return lax.ppermute(shard, PAIR, [(0, 1), (1, 0)])


def scaled(values, gain):
    mean = jnp.mean(values * values, axis=-1, keepdims=True)
    return values * lax.rsqrt(mean + epsilon) * gain


def silu(values):
    return values / (1.0 + jnp.exp(-values))


def in_vmem(values):
    return pltpu.with_memory_space_constraint(values, pltpu.VMEM)


def shifted(shard, step, members):
    pairs = []
    for core, sign in enumerate((1, -1)):
        for t in range(members):
            target = (t + sign * step) % members
            pairs.append((core * members + t, core * members + target))
    return lax.ppermute(shard, (PAIR, "tp"), pairs)


def wide_dot(left, right):
    return jnp.dot(left, right, preferred_element_type=jnp.float32)


def attend_kernel(*refs):
    inputs, outputs, scratch = refs[:20], refs[20:23], refs[23:]
    partial, packed, notes = outputs
    locals_, sems = scratch[:-1], scratch[-1]
    expert_gate, expert_up, expert_down, shared_down = inputs[16:]
    copies = []

    def start(source, target):
        copy = pltpu.make_async_copy(source, target, sems.at[len(copies)])
        copy.start()
        copies.append(copy)

    for source, target in zip(inputs[:16], locals_):
        start(source, target)
    tokens, norm_gain, query_weight, query_gain, key_weight, key_gain = locals_[:6]
    value_weight, forget_weight, forget_bias, keys, cum, lengths = locals_[6:12]
    values, out_weight, routes, route_weights = locals_[12:]
    first_packed = len(copies)
    row = 0

    def pack(source, row):
        start(source, packed.at[pl.ds(row, source.shape[0]), :])
        return row + source.shape[0]

    row = pack(expert_gate, row)
    row = pack(expert_up, row)
    for block in range(expert_down.shape[1] // LANES):
        row = pack(expert_down.at[:, pl.ds(block * LANES, LANES)], row)
    for block in range(shared_down.shape[1] // LANES):
        row = pack(shared_down.at[:, pl.ds(block * LANES, LANES)], row)

    seqs, cache_len, head = keys.shape
    groups = query_weight.shape[1] // head
    for copy in copies[:3]:
        copy.wait()
    normed = scaled(tokens[...].astype(jnp.float32), norm_gain[...].astype(jnp.float32))
    normed = normed.astype(jnp.bfloat16)
    for copy in copies[3:9]:
        copy.wait()
    gain = query_gain[...].astype(jnp.float32)
    wide = wide_dot(normed, query_weight[...])
    query = [scaled(wide[:, g * head : (g + 1) * head], gain) for g in range(groups)]
    query = jnp.concatenate(query, axis=0).astype(jnp.bfloat16)
    new_key = scaled(wide_dot(normed, key_weight[...]), key_gain[...].astype(jnp.float32))
    new_key = new_key.astype(jnp.bfloat16).astype(jnp.float32)
    new_value = wide_dot(normed, value_weight[...]).astype(jnp.bfloat16).astype(jnp.float32)
    products = normed.astype(jnp.float32) * forget_weight[...].astype(jnp.float32)
    forget = jnp.sum(products, axis=-1, keepdims=True) + forget_bias[0]
    new_log = jnp.minimum(forget, 0.0) - jnp.log1p(jnp.exp(-jnp.abs(forget)))

    rows = groups * seqs
    owner = lax.broadcasted_iota(jnp.int32, (rows, cache_len), 0) % seqs
    position = lax.broadcasted_iota(jnp.int32, (rows, cache_len), 1)
    scores = jnp.zeros((rows, cache_len), jnp.float32)
    decay = jnp.zeros((rows, cache_len), jnp.float32)
    length = jnp.zeros((rows, cache_len), jnp.int32)
    for copy in copies[9:12]:
        copy.wait()
    for b in range(seqs):
        mine = owner == b
        one = lax.dot_general(
            query, keys[b], (((1,), (1,)), ((), ())), preferred_element_type=jnp.float32
        )
        scores = jnp.where(mine, one, scores)
        decay = jnp.where(mine, cum[b], decay)
        length = jnp.where(mine, lengths[b], length)
    last = jnp.where(position == length - 1, decay, 0.0)
    last = jnp.sum(last, axis=-1, keepdims=True)
    bias = last - decay + jnp.concatenate([new_log] * groups, axis=0)
    score_scale = head ** (-0.5)
    past = jnp.where(position < length, scores * score_scale + bias, -jnp.inf)
    own = query.astype(jnp.float32) * jnp.concatenate([new_key] * groups, axis=0)
    own = jnp.sum(own, axis=-1, keepdims=True) * score_scale
    past_exp = jnp.exp(past)
    own_exp = jnp.exp(own)
    denominator = jnp.sum(past_exp, axis=-1, keepdims=True) + own_exp
    past_prob = (past_exp / denominator).astype(jnp.bfloat16)
    own_prob = (own_exp / denominator).astype(jnp.bfloat16).astype(jnp.float32)
    head_owner = owner[:, :head]
    mixed = jnp.zeros((rows, head), jnp.float32)
    copies[12].wait()
    for b in range(seqs):
        mixed = jnp.where(head_owner == b, wide_dot(past_prob, values[b]), mixed)
    mixed = mixed + own_prob * jnp.concatenate([new_value] * groups, axis=0)
    heads_out = [mixed[g * seqs : (g + 1) * seqs] for g in range(groups)]
    heads_out = jnp.concatenate(heads_out, axis=1).astype(jnp.bfloat16)
    copies[13].wait()
    product = wide_dot(heads_out, out_weight[...]).astype(jnp.bfloat16)
    for peer in range(partial.shape[0]):
        partial[peer] = product

    copies[14].wait()
    copies[15].wait()
    members = partial.shape[0]
    member = lax.axis_index("tp")
    norm_weights = route_weights[...]
    norm_weights = norm_weights / jnp.sum(norm_weights, axis=0, keepdims=True)
    high = norm_weights.astype(jnp.bfloat16).astype(jnp.float32)
    marks = (routes[...].astype(jnp.float32), high, norm_weights - high)
    column = lax.broadcasted_iota(jnp.int32, routes.shape, 1)
    lane = lax.broadcasted_iota(jnp.int32, (1, LANES), 1)
    lines = []
    for half in range(2):
        at = half * members + member
        line = jnp.zeros((1, LANES), jnp.float32)
        for i, mark in enumerate(marks):
            here = jnp.sum(jnp.where(column == at, mark, 0.0), axis=1, keepdims=True)
            for j in range(2):
                line = jnp.where(lane == 2 * i + j, here[j : j + 1], line)
        lines.append(line)
    notes[...] = jnp.concatenate(lines + [jnp.zeros((6, LANES), jnp.float32)], axis=0)
    for copy in copies[first_packed:]:
        copy.wait()


def rows_kernel(partial, tokens, ffn_gain, notes, residual, outgoing):
    member = lax.axis_index("tp")
    attended = jnp.sum(partial[...].astype(jnp.float32), axis=0)
    full = tokens[...].astype(jnp.float32) + attended
    seqs, width = full.shape
    members = partial.shape[0]
    slice_width = width // members
    for t in range(members):

        @pl.when(member == t)
        def _():
            residual[...] = full[:, t * slice_width : (t + 1) * slice_width]

    normed = scaled(full, ffn_gain[...].astype(jnp.float32))
    normed = normed.astype(jnp.bfloat16).astype(jnp.float32)
    rows_here = lax.broadcasted_iota(jnp.int32, (seqs, width), 0)
    pieces = []
    for half in range(2):
        at = half * members + member
        row = jnp.sum(jnp.where(rows_here == at, normed, 0.0), axis=0, keepdims=True)
        pieces += [row[:, k : k + LANES] for k in range(0, width, LANES)]
    pieces.append(notes[:2, :])
    pattern = jnp.concatenate(pieces * 8, axis=0).astype(jnp.bfloat16)
    step = pattern.shape[0]
    for i in range(outgoing.shape[0] // step):
        outgoing[i * step : (i + 1) * step, :] = pattern


def place_columns(target, values, n, depth, lines, blocks, per_member):
    for k in range(per_member):
        for line in range(lines):
            first = line // 2 * depth * 2 * blocks + n * depth * 2 * per_member
            first = first + line % 2 * per_member + k
            piece = values[line * depth : (line + 1) * depth, k * LANES : (k + 1) * LANES]
            target[pl.ds(first, depth, stride=2 * per_member), :] = piece


def hidden_of(values, pack, width):
    both = jnp.concatenate([pack[:width, :], pack[width : 2 * width, :]], axis=1)
    both = wide_dot(values, both)
    return (silu(both[:, :LANES]) * both[:, LANES:]).astype(jnp.bfloat16)


def down_of(packs, first, per_member):
    columns = []
    for k in range(per_member):
        rows = slice(first + k * LANES, first + (k + 1) * LANES)
        columns.append(jnp.concatenate([pack[rows, :] for pack in packs], axis=0))
    return jnp.concatenate(columns, axis=1)


def share_kernel(rows, front, pair_front, resident, *refs):
    sources, refs = refs[:-7], refs[-7:]
    out, narrow, aside, wide, columns, staged, sems = refs
    copies = []
    for i, source in enumerate(sources):
        copies.append(pltpu.make_async_copy(source, staged.at[i], sems.at[i]))
        copies[-1].start()
    members = lax.axis_size("tp")
    packs = [staged.at[i] for i in range(len(sources))]
    packs.insert(members, resident)
    member = lax.axis_index("tp")
    core = lax.axis_index(PAIR)
    experts = (lax.axis_index(EP), lax.axis_index(EP) + 1 - 2 * core)
    width = front.shape[1]
    count = narrow.shape[0]
    blocks = width // LANES
    stride = 2 * blocks + 2
    lines = lax.axis_size("ep_1") * 2
    depth = count // lines
    wide[: rows.shape[0], :] = rows[...].astype(jnp.float32)
    marks = []
    for line in range(lines):
        chip, half = line // 2, line % 2
        for k in range(blocks + 1):
            first = half * blocks + k if k < blocks else 2 * blocks + half
            piece = wide[pl.ds(chip * depth * stride + first, depth, stride=stride), :]
            if k < blocks:
                at = (slice(line * depth, (line + 1) * depth), slice(k * LANES, (k + 1) * LANES))
                narrow[at] = piece.astype(jnp.bfloat16)
            else:
                marks.append(piece)
    marks = jnp.concatenate(marks, axis=0)
    weights = []
    for expert in experts:
        weight = jnp.zeros((count, 1), jnp.float32)
        for j in range(2):
            norm_weight = marks[:, 2 + j : 3 + j] + marks[:, 4 + j : 5 + j]
            chosen = marks[:, j : j + 1] == expert.astype(jnp.float32)
            weight = weight + jnp.where(chosen, norm_weight, 0.0)
        weights.append(weight)
    values = narrow[...]
    down_start = 2 * width
    shared_start = down_start + blocks * LANES
    per_member = blocks // members
    units = (resident.shape[0] - shared_start) // per_member

    fronts = [
        lax.dot_general(
            values, each[...], (((1,), (1,)), ((), ())), preferred_element_type=jnp.float32
        )
        for each in (front, pair_front)
    ]
    mix_gate = 1.0 / (1.0 + jnp.exp(-fronts[0][:, 2 * units : 2 * units + 1]))
    shared = [silu(pre[:, :units]) * pre[:, units : 2 * units] for pre in fronts]
    shared = [each.astype(jnp.bfloat16) for each in shared]
    lane = lax.broadcasted_iota(jnp.int32, aside.shape, 1)
    scalars = jnp.where(lane == 0, weights[1], mix_gate)
    aside[...] = scalars
    aside[:, LANES - units :] = shared[1].astype(jnp.float32)

    hidden = []
    first_hidden = hidden_of(values, resident, width)
    for copy, pack in zip(copies, packs[:members] + packs[members + 1 :]):
        copy.wait()
        hidden.append(hidden_of(values, pack, width))
    hidden.insert(members, first_hidden)
    ahead = jnp.where(core == 0, members - 1, 1)
    origins = (0, ahead, members - ahead, 2)
    for s, pair in enumerate((0, 2, 1, None)):
        dense = wide_dot(shared[0], dense_of(packs[s], shared_start, units, per_member))
        if pair is not None:
            other = dense_of(packs[members + pair], shared_start, units, per_member)
            dense = dense + wide_dot(shared[1], other)
        columns[(member + origins[s]) % members] = mix_gate * dense
    for n in range(members):
        first = down_start + n * per_member * LANES
        total = columns[n]
        for side in range(2):
            routed = jnp.zeros((count, per_member * LANES), jnp.float32)
            for i in range(side * members, min((side + 1) * members, len(packs)), 2):
                group = packs[i : min(i + 2, len(packs))]
                left = jnp.concatenate(hidden[i : i + len(group)], axis=1)
                routed = routed + wide_dot(left, down_of(group, first, per_member))
            total = total + weights[side] * routed
        place_columns(out, total, n, depth, lines, blocks, per_member)


def dense_of(pack, shared_start, units, per_member):
    parts = [pack[pl.ds(shared_start + k * units, units), :] for k in range(per_member)]
    return jnp.concatenate(parts, axis=1)


def last_kernel(partial, narrow, aside, pack, out, wide, columns):
    members = lax.axis_size("tp")
    member = lax.axis_index("tp")
    count, width = narrow.shape
    blocks = width // LANES
    per_member = blocks // members
    lines = lax.axis_size("ep_1") * 2
    depth = count // lines
    down_start = 2 * width
    shared_start = down_start + blocks * LANES
    units = (pack.shape[0] - shared_start) // per_member
    weight = aside[:, 0:1]
    mix_gate = aside[:, 1:2]
    shared = aside[:, LANES - units :].astype(jnp.bfloat16)
    hidden = hidden_of(narrow[...], pack, width)
    dense = mix_gate * wide_dot(shared, dense_of(pack, shared_start, units, per_member))
    columns[...] = jnp.zeros(columns.shape, jnp.float32)
    columns[(member + 2) % members] = dense
    for n in range(members):
        first = down_start + n * per_member * LANES
        routed = wide_dot(hidden, down_of([pack], first, per_member))
        total = columns[n] + weight * routed
        place_columns(wide, total, n, depth, lines, blocks, per_member)
    out[...] = (partial[...] + wide[...]).astype(jnp.bfloat16)


def fold_kernel(parts, out, wide, small):
    sources = lax.axis_size("ep_1")
    members = lax.axis_size("tp")
    rows = parts.shape[0] // sources
    wide[...] = parts[...].astype(jnp.float32)
    total = wide[:rows, :]
    for i in range(1, sources):
        total = total + wide[i * rows : (i + 1) * rows, :]
    wide[:rows, :] = total
    halves = 2
    count = rows // members // halves
    for t in range(members):
        for j in range(halves):
            piece = wide[pl.ds(t * count * halves + j, count, stride=halves), :]
            small[pl.ds(t * halves + j, count, stride=members * halves), :] = piece
    out[...] = small[...].astype(jnp.bfloat16)


def finish_kernel(parts, residual, out, small):
    rows = small.shape[0]
    total = parts[:rows, :].astype(jnp.float32)
    for i in range(1, parts.shape[0] // rows):
        total = total + parts[i * rows : (i + 1) * rows, :].astype(jnp.float32)
    small[...] = total
    seqs = residual.shape[0]
    for j in range(rows // seqs):
        piece = small[pl.ds(j, seqs, stride=rows // seqs), :]
        columns = slice(j * LANES, (j + 1) * LANES)
        out[:, columns] = (residual[:, columns] + piece).astype(jnp.bfloat16)


def per_device(
    tokens,
    lengths,
    cache_keys,
    cache_values,
    cache_cum,
    norm_gain,
    query_weight,
    key_weight,
    value_weight,
    forget_weight,
    forget_bias,
    query_gain,
    key_gain,
    out_weight,
    ffn_gain,
    mix_weight,
    shared_gate,
    shared_up,
    shared_down,
    routes,
    route_weights,
    expert_gate,
    expert_up,
    expert_down,
):
    seqs, width = tokens.shape
    cache_len, head = cache_keys.shape[1], cache_keys.shape[3]
    peers = lax.axis_size(EP)
    members = lax.axis_size("tp")
    blocks = width // LANES
    units = shared_gate.shape[1]
    hidden = expert_gate.shape[2]
    pack_rows = 2 * width + hidden * blocks + units * shared_down.shape[1] // LANES
    copies = 2 + blocks + shared_down.shape[1] // LANES

    local = [
        tokens,
        norm_gain,
        query_weight,
        query_gain,
        key_weight,
        key_gain,
        value_weight,
        forget_weight.reshape(1, width),
        forget_bias,
        cache_keys.reshape(seqs, cache_len, head),
        cache_cum,
        lengths,
        cache_values.reshape(seqs, cache_len, head),
        out_weight,
        routes.T,
        route_weights.T,
    ]
    spaces = [pltpu.SMEM if each is forget_bias or each is lengths else pltpu.VMEM for each in local]
    partial, packed, notes = pl.pallas_call(
        attend_kernel,
        in_specs=[ANY] * (len(local) + 4),
        out_specs=[VMEM] * 3,
        out_shape=[
            pltpu.VMEM((members, seqs, width), jnp.bfloat16),
            pltpu.VMEM((pack_rows, LANES), jnp.bfloat16),
            pltpu.VMEM((8, LANES), jnp.float32),
        ],
        scratch_shapes=[space(each.shape, each.dtype) for space, each in zip(spaces, local)]
        + [pltpu.SemaphoreType.DMA((copies + len(local),))],
        name="attend",
    )(*local, expert_gate[0], expert_up[0], expert_down[0], shared_down)
    partial = lax.all_to_all(partial, "tp", 0, 0, tiled=True)
    ahead = shifted(packed, 1, members)
    behind = shifted(packed, -1, members)
    across = shifted(ahead, 1, members)
    packs = [packed, ahead, behind, across]

    front = [shared_gate.T, shared_up.T, mix_weight[None]]
    front = jnp.concatenate(front, axis=0)
    front = jnp.pad(front, ((0, LANES - front.shape[0]), (0, 0)))

    sub_rows = peers * (blocks + 1)
    sent_rows = sub_rows // lax.axis_size(EP[1])
    residual, outgoing = pl.pallas_call(
        rows_kernel,
        in_specs=[VMEM] * 4,
        out_specs=[VMEM, VMEM],
        out_shape=[
            pltpu.VMEM((seqs, width // members), jnp.float32),
            pltpu.VMEM((sent_rows, LANES), jnp.bfloat16),
        ],
        name="rows",
    )(*map(in_vmem, (partial, tokens, ffn_gain, notes)))
    column = lax.all_to_all(outgoing.reshape(-1, 2, LANES), EP[0], 0, 0, tiled=True)
    copies_out = jnp.tile(column, (lax.axis_size(EP[1]), 1, 1))
    own_rows = lax.all_to_all(copies_out, EP[1], 0, 0, tiled=True)


    pair_front = swap(front)
    pair_packs = []
    for pack in packs:
        pair_packs.append(swap(pack))
    streamed = packs + pair_packs[1:-1]
    local_columns = pltpu.VMEM((members, peers, width // members), jnp.float32)
    partial_share, narrow, aside = pl.pallas_call(
        share_kernel,
        in_specs=[VMEM] * 4 + [ANY] * len(streamed),
        out_specs=[VMEM] * 3,
        out_shape=[
            pltpu.VMEM((peers * blocks, LANES), jnp.float32),
            pltpu.VMEM((peers, width), jnp.bfloat16),
            pltpu.VMEM((peers, LANES), jnp.float32),
        ],
        scratch_shapes=[
            pltpu.VMEM((sub_rows, LANES), jnp.float32),
            local_columns,
            pltpu.VMEM((len(streamed), pack_rows, LANES), jnp.bfloat16),
            pltpu.SemaphoreType.DMA((len(streamed),)),
        ],
        name="share",
    )(
        *map(in_vmem, (own_rows.reshape(sub_rows, LANES), front, pair_front, pair_packs[0])),
        *streamed,
    )
    total = pl.pallas_call(
        last_kernel,
        in_specs=[VMEM] * 4,
        out_specs=VMEM,
        out_shape=pltpu.VMEM((peers * blocks, LANES), jnp.bfloat16),
        scratch_shapes=[pltpu.VMEM((peers * blocks, LANES), jnp.float32), local_columns],
        name="last",
    )(*map(in_vmem, (partial_share, narrow, aside)), pair_packs[-1])
    parts = lax.all_to_all(total.reshape(-1, 2, LANES), ("ep_1", "tp"), 0, 0, tiled=True)
    parts = parts.reshape(-1, LANES)
    rows = parts.shape[0] // lax.axis_size("ep_1")
    parts = pl.pallas_call(
        fold_kernel,
        in_specs=[VMEM],
        out_specs=VMEM,
        out_shape=pltpu.VMEM((rows, LANES), jnp.bfloat16),
        scratch_shapes=[
            pltpu.VMEM(parts.shape, jnp.float32),
            pltpu.VMEM((rows, LANES), jnp.float32),
        ],
        name="fold",
    )(in_vmem(parts))
    parts = lax.all_to_all(parts.reshape(-1, 2, LANES), EP[0], 0, 0, tiled=True)
    return pl.pallas_call(
        finish_kernel,
        in_specs=[VMEM] * 2,
        out_specs=VMEM,
        out_shape=jax.ShapeDtypeStruct((seqs, width // members), jnp.bfloat16),
        scratch_shapes=[pltpu.VMEM((seqs * width // members // LANES, LANES), jnp.float32)],
        name="finish",
    )(in_vmem(parts.reshape(-1, LANES)), in_vmem(residual))


def solution(mesh):
    finer = Mesh(mesh.devices.reshape(16, 4, 2, mesh.shape["tp"]), ("ep_0", "ep_1", "ep_2", "tp"))
    placed = (
        P(EP, None),
        P(EP),
        P(EP, None, "tp", None),
        P(EP, None, "tp", None),
        P(EP, "tp", None),
        P(),
        P(None, "tp"),
        P(None, "tp"),
        P(None, "tp"),
        P(None, "tp"),
        P("tp"),
        P(),
        P(),
        P("tp", None),
        P(),
        P(),
        P(None, EP),
        P(None, EP),
        P(EP, "tp"),
        P(EP, None),
        P(EP, None),
        P(EP, None, "tp"),
        P(EP, None, "tp"),
        P(EP, "tp", None),
    )

    return jax.shard_map(
        per_device, mesh=finer, in_specs=placed, out_specs=P(EP, "tp"), check_vma=False
    )
```

```python
import jax
import jax.numpy as jnp
from jax import lax
from jax.experimental import pallas as pl
from jax.experimental.pallas import tpu as pltpu
from jax.sharding import Mesh
from jax.sharding import PartitionSpec as P

EP = ("ep_0", "ep_1", "ep_2")
PAIR = "ep_2"
LANES = 128

epsilon = 1e-06

VMEM = pl.BlockSpec(memory_space=pltpu.VMEM)
SMEM = pl.BlockSpec(memory_space=pltpu.SMEM)
ANY = pl.BlockSpec(memory_space=pl.ANY)


def swap(shard):
    return lax.ppermute(shard, PAIR, [(0, 1), (1, 0)])


def scaled(values, gain):
    mean = jnp.mean(values * values, axis=-1, keepdims=True)
    return values * lax.rsqrt(mean + epsilon) * gain


def silu(values):
    return values / (1.0 + jnp.exp(-values))


def in_vmem(values):
    return pltpu.with_memory_space_constraint(values, pltpu.VMEM)


def shifted(shard, step, members):
    pairs = []
    for core, sign in enumerate((1, -1)):
        for t in range(members):
            target = (t + sign * step) % members
            pairs.append((core * members + t, core * members + target))
    return lax.ppermute(shard, (PAIR, "tp"), pairs)


def wide_dot(left, right):
    return jnp.dot(left, right, preferred_element_type=jnp.float32)


def attend_kernel(*refs):
    inputs, outputs, scratch = refs[:20], refs[20:23], refs[23:]
    partial, packed, notes = outputs
    locals_, sems = scratch[:-1], scratch[-1]
    expert_gate, expert_up, expert_down, shared_down = inputs[16:]
    copies = []

    def start(source, target):
        copy = pltpu.make_async_copy(source, target, sems.at[len(copies)])
        copy.start()
        copies.append(copy)

    for source, target in zip(inputs[:16], locals_):
        start(source, target)
    tokens, norm_gain, query_weight, query_gain, key_weight, key_gain = locals_[:6]
    value_weight, forget_weight, forget_bias, keys, cum, lengths = locals_[6:12]
    values, out_weight, routes, route_weights = locals_[12:]
    first_packed = len(copies)
    row = 0

    def pack(source, row):
        start(source, packed.at[pl.ds(row, source.shape[0]), :])
        return row + source.shape[0]

    row = pack(expert_gate, row)
    row = pack(expert_up, row)
    for block in range(expert_down.shape[1] // LANES):
        row = pack(expert_down.at[:, pl.ds(block * LANES, LANES)], row)
    for block in range(shared_down.shape[1] // LANES):
        row = pack(shared_down.at[:, pl.ds(block * LANES, LANES)], row)

    seqs, cache_len, head = keys.shape
    groups = query_weight.shape[1] // head
    for copy in copies[:3]:
        copy.wait()
    normed = scaled(tokens[...].astype(jnp.float32), norm_gain[...].astype(jnp.float32))
    normed = normed.astype(jnp.bfloat16)
    for copy in copies[3:9]:
        copy.wait()
    gain = query_gain[...].astype(jnp.float32)
    wide = wide_dot(normed, query_weight[...])
    query = [scaled(wide[:, g * head : (g + 1) * head], gain) for g in range(groups)]
    query = jnp.concatenate(query, axis=0).astype(jnp.bfloat16)
    new_key = scaled(wide_dot(normed, key_weight[...]), key_gain[...].astype(jnp.float32))
    new_key = new_key.astype(jnp.bfloat16).astype(jnp.float32)
    new_value = wide_dot(normed, value_weight[...]).astype(jnp.bfloat16).astype(jnp.float32)
    products = normed.astype(jnp.float32) * forget_weight[...].astype(jnp.float32)
    forget = jnp.sum(products, axis=-1, keepdims=True) + forget_bias[0]
    new_log = jnp.minimum(forget, 0.0) - jnp.log1p(jnp.exp(-jnp.abs(forget)))

    rows = groups * seqs
    owner = lax.broadcasted_iota(jnp.int32, (rows, cache_len), 0) % seqs
    position = lax.broadcasted_iota(jnp.int32, (rows, cache_len), 1)
    scores = jnp.zeros((rows, cache_len), jnp.float32)
    decay = jnp.zeros((rows, cache_len), jnp.float32)
    length = jnp.zeros((rows, cache_len), jnp.int32)
    for copy in copies[9:12]:
        copy.wait()
    for b in range(seqs):
        mine = owner == b
        one = lax.dot_general(
            query, keys[b], (((1,), (1,)), ((), ())), preferred_element_type=jnp.float32
        )
        scores = jnp.where(mine, one, scores)
        decay = jnp.where(mine, cum[b], decay)
        length = jnp.where(mine, lengths[b], length)
    last = jnp.where(position == length - 1, decay, 0.0)
    last = jnp.sum(last, axis=-1, keepdims=True)
    bias = last - decay + jnp.concatenate([new_log] * groups, axis=0)
    score_scale = head ** (-0.5)
    past = jnp.where(position < length, scores * score_scale + bias, -jnp.inf)
    own = query.astype(jnp.float32) * jnp.concatenate([new_key] * groups, axis=0)
    own = jnp.sum(own, axis=-1, keepdims=True) * score_scale
    past_exp = jnp.exp(past)
    own_exp = jnp.exp(own)
    denominator = jnp.sum(past_exp, axis=-1, keepdims=True) + own_exp
    past_prob = (past_exp / denominator).astype(jnp.bfloat16)
    own_prob = (own_exp / denominator).astype(jnp.bfloat16).astype(jnp.float32)
    head_owner = owner[:, :head]
    mixed = jnp.zeros((rows, head), jnp.float32)
    copies[12].wait()
    for b in range(seqs):
        mixed = jnp.where(head_owner == b, wide_dot(past_prob, values[b]), mixed)
    mixed = mixed + own_prob * jnp.concatenate([new_value] * groups, axis=0)
    heads_out = [mixed[g * seqs : (g + 1) * seqs] for g in range(groups)]
    heads_out = jnp.concatenate(heads_out, axis=1).astype(jnp.bfloat16)
    copies[13].wait()
    product = wide_dot(heads_out, out_weight[...]).astype(jnp.bfloat16)
    for peer in range(partial.shape[0]):
        partial[peer] = product

    copies[14].wait()
    copies[15].wait()
    members = partial.shape[0]
    member = lax.axis_index("tp")
    norm_weights = route_weights[...]
    norm_weights = norm_weights / jnp.sum(norm_weights, axis=0, keepdims=True)
    high = norm_weights.astype(jnp.bfloat16).astype(jnp.float32)
    marks = (routes[...].astype(jnp.float32), high, norm_weights - high)
    column = lax.broadcasted_iota(jnp.int32, routes.shape, 1)
    lane = lax.broadcasted_iota(jnp.int32, (1, LANES), 1)
    lines = []
    for half in range(2):
        at = half * members + member
        line = jnp.zeros((1, LANES), jnp.float32)
        for i, mark in enumerate(marks):
            here = jnp.sum(jnp.where(column == at, mark, 0.0), axis=1, keepdims=True)
            for j in range(2):
                line = jnp.where(lane == 2 * i + j, here[j : j + 1], line)
        lines.append(line)
    notes[...] = jnp.concatenate(lines + [jnp.zeros((6, LANES), jnp.float32)], axis=0)
    for copy in copies[first_packed:]:
        copy.wait()


def rows_kernel(partial, tokens, ffn_gain, notes, residual, outgoing):
    member = lax.axis_index("tp")
    attended = jnp.sum(partial[...].astype(jnp.float32), axis=0)
    full = tokens[...].astype(jnp.float32) + attended
    seqs, width = full.shape
    members = partial.shape[0]
    slice_width = width // members
    for t in range(members):

        @pl.when(member == t)
        def _():
            residual[...] = full[:, t * slice_width : (t + 1) * slice_width]

    normed = scaled(full, ffn_gain[...].astype(jnp.float32))
    normed = normed.astype(jnp.bfloat16).astype(jnp.float32)
    rows_here = lax.broadcasted_iota(jnp.int32, (seqs, width), 0)
    pieces = []
    for half in range(2):
        at = half * members + member
        row = jnp.sum(jnp.where(rows_here == at, normed, 0.0), axis=0, keepdims=True)
        pieces += [row[:, k : k + LANES] for k in range(0, width, LANES)]
    pieces.append(notes[:2, :])
    pattern = jnp.concatenate(pieces * 8, axis=0).astype(jnp.bfloat16)
    step = pattern.shape[0]
    for i in range(outgoing.shape[0] // step):
        outgoing[i * step : (i + 1) * step, :] = pattern


def place_columns(target, values, n, depth, lines, blocks, per_member):
    for k in range(per_member):
        for line in range(lines):
            first = line // 2 * depth * 2 * blocks + n * depth * 2 * per_member
            first = first + line % 2 * per_member + k
            piece = values[line * depth : (line + 1) * depth, k * LANES : (k + 1) * LANES]
            target[pl.ds(first, depth, stride=2 * per_member), :] = piece


def hidden_of(values, pack, width):
    both = jnp.concatenate([pack[:width, :], pack[width : 2 * width, :]], axis=1)
    both = wide_dot(values, both)
    return (silu(both[:, :LANES]) * both[:, LANES:]).astype(jnp.bfloat16)


def down_of(packs, first, per_member):
    columns = []
    for k in range(per_member):
        rows = slice(first + k * LANES, first + (k + 1) * LANES)
        columns.append(jnp.concatenate([pack[rows, :] for pack in packs], axis=0))
    return jnp.concatenate(columns, axis=1)


def share_kernel(rows, front, pair_front, *refs):
    sources, refs = refs[:-7], refs[-7:]
    out, narrow, aside, wide, columns, staged, sems = refs
    copies = []
    for i, source in enumerate(sources):
        copies.append(pltpu.make_async_copy(source, staged.at[i], sems.at[i]))
    members = lax.axis_size("tp")
    packs = [staged.at[i] for i in range(len(sources))]
    member = lax.axis_index("tp")
    core = lax.axis_index(PAIR)
    for copy in copies:
        copy.start()
    experts = (lax.axis_index(EP), lax.axis_index(EP) + 1 - 2 * core)
    width = front.shape[1]
    count = narrow.shape[0]
    blocks = width // LANES
    stride = 2 * blocks + 2
    lines = lax.axis_size("ep_1") * 2
    depth = count // lines
    wide[: rows.shape[0], :] = rows[...].astype(jnp.float32)
    marks = []
    for line in range(lines):
        chip, half = line // 2, line % 2
        for k in range(blocks + 1):
            first = chip * stride + (half * blocks + k if k < blocks else 2 * blocks + half)
            piece = wide[pl.ds(first, depth, stride=lines // 2 * stride), :]
            if k < blocks:
                at = (slice(line * depth, (line + 1) * depth), slice(k * LANES, (k + 1) * LANES))
                narrow[at] = piece.astype(jnp.bfloat16)
            else:
                marks.append(piece)
    marks = jnp.concatenate(marks, axis=0)
    weights = []
    for expert in experts:
        weight = jnp.zeros((count, 1), jnp.float32)
        for j in range(2):
            norm_weight = marks[:, 2 + j : 3 + j] + marks[:, 4 + j : 5 + j]
            chosen = marks[:, j : j + 1] == expert.astype(jnp.float32)
            weight = weight + jnp.where(chosen, norm_weight, 0.0)
        weights.append(weight)
    values = narrow[...]
    down_start = 2 * width
    shared_start = down_start + blocks * LANES
    per_member = blocks // members
    units = (packs[0].shape[0] - shared_start) // per_member

    fronts = [
        lax.dot_general(
            values, each[...], (((1,), (1,)), ((), ())), preferred_element_type=jnp.float32
        )
        for each in (front, pair_front)
    ]
    mix_gate = 1.0 / (1.0 + jnp.exp(-fronts[0][:, 2 * units : 2 * units + 1]))
    shared = [silu(pre[:, :units]) * pre[:, units : 2 * units] for pre in fronts]
    shared = [each.astype(jnp.bfloat16) for each in shared]
    lane = lax.broadcasted_iota(jnp.int32, aside.shape, 1)
    scalars = jnp.where(lane == 0, weights[1], mix_gate)
    aside[...] = scalars
    aside[:, LANES - units :] = shared[1].astype(jnp.float32)

    hidden = []
    for copy, pack in zip(copies, packs):
        copy.wait()
        hidden.append(hidden_of(values, pack, width))
    ahead = jnp.where(core == 0, members - 1, 1)
    origins = (0, ahead, members - ahead, 2)
    for s, pair in enumerate((0, 2, 1, None)):
        dense = wide_dot(shared[0], dense_of(packs[s], shared_start, units, per_member))
        if pair is not None:
            other = dense_of(packs[members + pair], shared_start, units, per_member)
            dense = dense + wide_dot(shared[1], other)
        columns[(member + origins[s]) % members] = mix_gate * dense
    for n in range(members):
        first = down_start + n * per_member * LANES
        total = columns[n]
        for side in range(2):
            routed = jnp.zeros((count, per_member * LANES), jnp.float32)
            for i in range(side * members, min((side + 1) * members, len(packs)), 2):
                group = packs[i : min(i + 2, len(packs))]
                left = jnp.concatenate(hidden[i : i + len(group)], axis=1)
                routed = routed + wide_dot(left, down_of(group, first, per_member))
            total = total + weights[side] * routed
        place_columns(out, total, n, depth, lines, blocks, per_member)


def dense_of(pack, shared_start, units, per_member):
    parts = [pack[pl.ds(shared_start + k * units, units), :] for k in range(per_member)]
    return jnp.concatenate(parts, axis=1)


def last_kernel(partial, narrow, aside, pack, out, wide, columns):
    members = lax.axis_size("tp")
    member = lax.axis_index("tp")
    count, width = narrow.shape
    blocks = width // LANES
    per_member = blocks // members
    lines = lax.axis_size("ep_1") * 2
    depth = count // lines
    down_start = 2 * width
    shared_start = down_start + blocks * LANES
    units = (pack.shape[0] - shared_start) // per_member
    weight = aside[:, 0:1]
    mix_gate = aside[:, 1:2]
    shared = aside[:, LANES - units :].astype(jnp.bfloat16)
    hidden = hidden_of(narrow[...], pack, width)
    dense = mix_gate * wide_dot(shared, dense_of(pack, shared_start, units, per_member))
    columns[...] = jnp.zeros(columns.shape, jnp.float32)
    columns[(member + 2) % members] = dense
    for n in range(members):
        first = down_start + n * per_member * LANES
        routed = wide_dot(hidden, down_of([pack], first, per_member))
        total = columns[n] + weight * routed
        place_columns(wide, total, n, depth, lines, blocks, per_member)
    out[...] = (partial[...] + wide[...]).astype(jnp.bfloat16)


def fold_kernel(parts, out, wide, small):
    sources = lax.axis_size("ep_1")
    members = lax.axis_size("tp")
    rows = parts.shape[0] // sources
    wide[...] = parts[...].astype(jnp.float32)
    total = wide[:rows, :]
    for i in range(1, sources):
        total = total + wide[i * rows : (i + 1) * rows, :]
    wide[:rows, :] = total
    halves = 2
    count = rows // members // halves
    for t in range(members):
        for j in range(halves):
            piece = wide[pl.ds(t * count * halves + j, count, stride=halves), :]
            small[pl.ds(t * halves + j, count, stride=members * halves), :] = piece
    out[...] = small[...].astype(jnp.bfloat16)


def finish_kernel(parts, residual, out, small):
    rows = small.shape[0]
    total = parts[:rows, :].astype(jnp.float32)
    for i in range(1, parts.shape[0] // rows):
        total = total + parts[i * rows : (i + 1) * rows, :].astype(jnp.float32)
    small[...] = total
    seqs = residual.shape[0]
    for j in range(rows // seqs):
        piece = small[pl.ds(j, seqs, stride=rows // seqs), :]
        columns = slice(j * LANES, (j + 1) * LANES)
        out[:, columns] = (residual[:, columns] + piece).astype(jnp.bfloat16)


def per_device(
    tokens,
    lengths,
    cache_keys,
    cache_values,
    cache_cum,
    norm_gain,
    query_weight,
    key_weight,
    value_weight,
    forget_weight,
    forget_bias,
    query_gain,
    key_gain,
    out_weight,
    ffn_gain,
    mix_weight,
    shared_gate,
    shared_up,
    shared_down,
    routes,
    route_weights,
    expert_gate,
    expert_up,
    expert_down,
):
    seqs, width = tokens.shape
    cache_len, head = cache_keys.shape[1], cache_keys.shape[3]
    peers = lax.axis_size(EP)
    members = lax.axis_size("tp")
    blocks = width // LANES
    units = shared_gate.shape[1]
    hidden = expert_gate.shape[2]
    pack_rows = 2 * width + hidden * blocks + units * shared_down.shape[1] // LANES
    copies = 2 + blocks + shared_down.shape[1] // LANES

    local = [
        tokens,
        norm_gain,
        query_weight,
        query_gain,
        key_weight,
        key_gain,
        value_weight,
        forget_weight.reshape(1, width),
        forget_bias,
        cache_keys.reshape(seqs, cache_len, head),
        cache_cum,
        lengths,
        cache_values.reshape(seqs, cache_len, head),
        out_weight,
        routes.T,
        route_weights.T,
    ]
    spaces = [pltpu.SMEM if each is forget_bias or each is lengths else pltpu.VMEM for each in local]
    partial, packed, notes = pl.pallas_call(
        attend_kernel,
        in_specs=[ANY] * (len(local) + 4),
        out_specs=[VMEM] * 3,
        out_shape=[
            pltpu.VMEM((members, seqs, width), jnp.bfloat16),
            pltpu.VMEM((pack_rows, LANES), jnp.bfloat16),
            pltpu.VMEM((8, LANES), jnp.float32),
        ],
        scratch_shapes=[space(each.shape, each.dtype) for space, each in zip(spaces, local)]
        + [pltpu.SemaphoreType.DMA((copies + len(local),))],
        name="attend",
    )(*local, expert_gate[0], expert_up[0], expert_down[0], shared_down)
    partial = lax.all_to_all(partial, "tp", 0, 0, tiled=True)
    ahead = shifted(packed, 1, members)
    behind = shifted(packed, -1, members)
    across = shifted(ahead, 1, members)
    packs = [packed, ahead, behind, across]

    front = [shared_gate.T, shared_up.T, mix_weight[None]]
    front = jnp.concatenate(front, axis=0)
    front = jnp.pad(front, ((0, LANES - front.shape[0]), (0, 0)))

    sub_rows = peers * (blocks + 1)
    residual, outgoing = pl.pallas_call(
        rows_kernel,
        in_specs=[VMEM] * 4,
        out_specs=[VMEM, VMEM],
        out_shape=[
            pltpu.VMEM((seqs, width // members), jnp.float32),
            pltpu.VMEM((sub_rows, LANES), jnp.bfloat16),
        ],
        name="rows",
    )(*map(in_vmem, (partial, tokens, ffn_gain, notes)))
    own_rows = lax.all_to_all(outgoing.reshape(-1, 2, LANES), EP[:2], 0, 0, tiled=True)


    pair_front = swap(front)
    pair_packs = []
    for pack in packs:
        pair_packs.append(swap(pack))
    streamed = packs + pair_packs[:-1]
    local_columns = pltpu.VMEM((members, peers, width // members), jnp.float32)
    partial_share, narrow, aside = pl.pallas_call(
        share_kernel,
        in_specs=[VMEM] * 3 + [ANY] * len(streamed),
        out_specs=[VMEM] * 3,
        out_shape=[
            pltpu.VMEM((peers * blocks, LANES), jnp.float32),
            pltpu.VMEM((peers, width), jnp.bfloat16),
            pltpu.VMEM((peers, LANES), jnp.float32),
        ],
        scratch_shapes=[
            pltpu.VMEM((sub_rows, LANES), jnp.float32),
            local_columns,
            pltpu.VMEM((len(streamed), pack_rows, LANES), jnp.bfloat16),
            pltpu.SemaphoreType.DMA((len(streamed),)),
        ],
        name="share",
    )(
        *map(in_vmem, (own_rows.reshape(sub_rows, LANES), front, pair_front)),
        *streamed,
    )
    total = pl.pallas_call(
        last_kernel,
        in_specs=[VMEM] * 4,
        out_specs=VMEM,
        out_shape=pltpu.VMEM((peers * blocks, LANES), jnp.bfloat16),
        scratch_shapes=[pltpu.VMEM((peers * blocks, LANES), jnp.float32), local_columns],
        name="last",
    )(*map(in_vmem, (partial_share, narrow, aside)), pair_packs[-1])
    parts = lax.all_to_all(total.reshape(-1, 2, LANES), ("ep_1", "tp"), 0, 0, tiled=True)
    parts = parts.reshape(-1, LANES)
    rows = parts.shape[0] // lax.axis_size("ep_1")
    parts = pl.pallas_call(
        fold_kernel,
        in_specs=[VMEM],
        out_specs=VMEM,
        out_shape=pltpu.VMEM((rows, LANES), jnp.bfloat16),
        scratch_shapes=[
            pltpu.VMEM(parts.shape, jnp.float32),
            pltpu.VMEM((rows, LANES), jnp.float32),
        ],
        name="fold",
    )(in_vmem(parts))
    parts = lax.all_to_all(parts.reshape(-1, 2, LANES), EP[0], 0, 0, tiled=True)
    return pl.pallas_call(
        finish_kernel,
        in_specs=[VMEM] * 2,
        out_specs=VMEM,
        out_shape=jax.ShapeDtypeStruct((seqs, width // members), jnp.bfloat16),
        scratch_shapes=[pltpu.VMEM((seqs * width // members // LANES, LANES), jnp.float32)],
        name="finish",
    )(in_vmem(parts.reshape(-1, LANES)), in_vmem(residual))


def solution(mesh):
    finer = Mesh(mesh.devices.reshape(16, 4, 2, mesh.shape["tp"]), ("ep_0", "ep_1", "ep_2", "tp"))
    placed = (
        P(EP, None),
        P(EP),
        P(EP, None, "tp", None),
        P(EP, None, "tp", None),
        P(EP, "tp", None),
        P(),
        P(None, "tp"),
        P(None, "tp"),
        P(None, "tp"),
        P(None, "tp"),
        P("tp"),
        P(),
        P(),
        P("tp", None),
        P(),
        P(),
        P(None, EP),
        P(None, EP),
        P(EP, "tp"),
        P(EP, None),
        P(EP, None),
        P(EP, None, "tp"),
        P(EP, None, "tp"),
        P(EP, "tp", None),
    )

    return jax.shard_map(
        per_device, mesh=finer, in_specs=placed, out_specs=P(EP, "tp"), check_vma=False
    )
```
